32 devices in a mesh: ep: 8 (over z, x), tp: 4 (over y, core).
Axes of the slice: x: 2, y: 2, z: 4, core: 2. Of those that a mesh axis runs over, the one named last changes fastest.
Arguments:
- mix_rows: bfloat16 [2048, 2048], P('ep'), may hold values from -6 to 6
- mix_gain: bfloat16 [2048], replicated, may hold values from 0.099609375 to 1.8984375
- w_query: bfloat16 [1024, 2048], P('tp'), may hold values from -0.125 to 0.125
- w_key: bfloat16 [1024, 2048], P('tp'), may hold values from -0.125 to 0.125
- w_value: bfloat16 [1024, 2048], P('tp'), may hold values from -0.125 to 0.125
- key_offset: float32 [16, 2048], P('tp'), may hold values from -11 to 0
- w_out: bfloat16 [1024, 2048], P('tp'), may hold values from -0.1875 to 0.1875
- out_gain: bfloat16 [2048], replicated, may hold values from 0.099609375 to 1.8984375
- exp_rows: bfloat16 [768, 2048], P('ep', 'tp'), may hold values from -100 to 100
- exp_gain: bfloat16 [2048], P('tp'), may hold values from 0.099609375 to 1.8984375
- routes: int32 [768, 4], P('ep'), may hold values from 0 to 7, all different within a row; in each aligned block of 96 rows (0 to 95, 96 to 191, ...) at most 64 rows name the same one
- route_weight: float32 [768, 4], P('ep'), may hold values from 0.05 to 1
- w_gate: bfloat16 [8, 2048, 2048], P('ep', None, 'tp'), may hold values from -0.5 to 0.5
- w_up: bfloat16 [8, 2048, 2048], P('ep', None, 'tp'), may hold values from -0.5 to 0.5
- w_down: bfloat16 [8, 2048, 2048], P('ep', 'tp'), may hold values from -0.1875 to 0.1875
Outputs:
- mix_out: bfloat16 [2048, 2048], P('ep')
- exp_out: bfloat16 [768, 2048], P('ep', 'tp')
The draws below stay inside these ranges and needn't reach their ends.
Inputs may be any that keep to these rules, and one draw needn't show every extreme that they name: `routes`: each row names 4 different experts. Within the rows of one device (aligned blocks of 96 rows) no expert is named by more than 64 rows, and in some blocks one expert is named by exactly 64 rows.
All inputs are finite; a program needn't handle non-finite values.
Results may differ from the reference program's by a relative error of at most 0.019.
Values may be sent and summed in bfloat16 or wider, within the bound.
A program may use at most 128 MiB of HBM per device.

```python
import math
import jax
import jax.numpy as jnp
import numpy as np
from jax import lax

D = 2048
ATTENTION_HEADS = 16
HEAD = 64
FF = 2048
TOPK = 4
MIX_ROWS = 256
EXP_ROWS = 96
EXPERTS = 8
CAP = 64
FF_PART = 512
ATT = 1024
SEQ_LEN = 2048
TOK_B = 768


def draw_key_offset(key, part):
    starting_key = jax.random.fold_in(key, 101)
    level_key, displacement_key, jitter_key = jax.random.split(starting_key, 3)
    lowest_reach = 0.6
    highest_reach = 1.6
    chain_reach = jax.random.uniform(level_key, (ATTENTION_HEADS, 1), minval=lowest_reach, maxval=highest_reach)
    head_level = jnp.log(chain_reach / SEQ_LEN) - 0.5
    block_shift = jax.random.uniform(displacement_key, (ATTENTION_HEADS, SEQ_LEN // MIX_ROWS), minval=-0.7, maxval=0.7)
    jitter = jax.random.uniform(jitter_key, (ATTENTION_HEADS, SEQ_LEN), minval=-0.5, maxval=0.5)
    offset_values = head_level + jnp.repeat(block_shift, MIX_ROWS, axis=1) + jitter
    return jnp.clip(offset_values, -11.0, 0.0).astype(jnp.float32)


def draw_exp_rows(key, part):
    starting_key = jax.random.fold_in(key, 202)
    noise_key = jax.random.fold_in(starting_key, 0)
    profile = jnp.exp(jnp.linspace(0.0, math.log(6.0), D))[None, :]
    noise = jnp.clip(jax.random.normal(noise_key, (TOK_B, D), jnp.float32), -5.0, 5.0)
    numbers = noise * profile
    return jnp.clip(numbers, -100.0, 100.0).astype(jnp.bfloat16)


def clamp_weights(key, salt):
    starting_key = jax.random.fold_in(key, salt)
    noise_key = jax.random.fold_in(starting_key, 0)
    noise = jnp.clip(jax.random.normal(noise_key, (EXPERTS, D, FF), jnp.float32), -5.0, 5.0) * D ** (-0.5)
    factor = 2.0
    return jnp.clip(noise * factor, -0.5, 0.5).astype(jnp.bfloat16)


def draw_w_gate(key, part):
    return clamp_weights(key, 303)


def draw_w_up(key, part):
    return clamp_weights(key, 404)


def with_spikes(entries, own_key, source, target, shards_of, factor):
    def block_of(position):
        return (jnp.arange(entries.shape[position]) // (entries.shape[position] // shards_of)).reshape((-1,) + (1,) * (entries.ndim - 1 - position))

    first = jax.random.permutation(own_key, shards_of)[block_of(target)]
    other_side = (block_of(target) + shards_of // 2) % shards_of
    return jnp.where((block_of(source) == first) | (block_of(source) == other_side), factor * entries, entries)


def block_scale(rng, extent, cuts, low, high):
    level = 1.0
    for axis_at, shards_of in cuts:
        draws = jax.random.uniform(jax.random.fold_in(jax.random.fold_in(rng, 6), axis_at), (shards_of,), jnp.float32, low / len(cuts), high / len(cuts))
        level = level * jnp.repeat(jnp.exp(draws), extent[axis_at] // shards_of).reshape((-1,) + (1,) * (len(extent) - 1 - axis_at))
    return level


def routed_block(key, own, number, rows, count, top, most, slope):
    ranking = jax.random.permutation(key, count)
    crowded, ordinary = load_shares(count, rows * top, most, slope, True), load_shares(count, rows * top, most, slope, False)
    places = jnp.arange(count)

    def named(sizes, rotation):
        used = int((sizes > 0).sum())
        fixed = max(1, used // 4)
        passed = fixed + (places - fixed + rotation * (used - fixed)) % max(1, count - fixed)
        return jnp.zeros((count,), jnp.int32).at[ranking[jnp.where(places < fixed, places, passed)]].set(jnp.asarray(sizes, jnp.int32))

    sizes = jnp.where(number % 4 == 0, named(crowded, number // 4), named(ordinary, number - number // 4 - 1))
    mixed = jax.random.permutation(jax.random.fold_in(own, 3), count)
    giver, sink = mixed[0:count // 2 * 2:2], mixed[1:count // 2 * 2:2]
    slack = jnp.minimum(sizes[giver] - 1, most - sizes[sink]) // 2
    slack = jnp.where((giver == ranking[0]) | (sink == ranking[0]) | (sizes[sink] == 0), 0, jnp.maximum(slack, 0))
    passed = jax.random.randint(jax.random.fold_in(own, 4), (count // 2,), 0, 1 << 20) % (slack + 1)
    sizes = sizes.at[giver].add(-passed).at[sink].add(passed)
    labels = jnp.searchsorted(jnp.cumsum(sizes), jnp.arange(rows * top), side="right").astype(jnp.int32)
    listing = labels.reshape(top, rows).T
    listing = listing[jax.random.permutation(jax.random.fold_in(own, 1), rows)]
    rotation = jax.random.randint(jax.random.fold_in(own, 2), (rows, 1), 0, top)
    return jnp.take_along_axis(listing, (jnp.arange(top)[None, :] + rotation) % top, axis=1)


def load_shares(amount, total, limit, skew, full):
    portions = [(1 << 20) // math.isqrt(rank ** skew) + 1 for rank in range(1, amount + 1)]
    largest = limit if full else min(limit, max(-(-total // amount), total * portions[0] // sum(portions)))
    least = 1 if total - largest >= amount - 1 else 0
    counts, rest = [largest] + [least] * (amount - 1), total - largest - least * (amount - 1)
    while rest > 0:
        free = [i for i in range(1, amount) if counts[i] < largest] or [i for i in range(1, amount) if counts[i] < limit]
        pool, remaining = sum([portions[i] for i in free]), rest
        for i in free:
            extra = min(limit - counts[i], max(1, remaining * portions[i] // pool), rest)
            counts[i] = counts[i] + extra
            rest = rest - extra
    return np.array(counts)


def bell_draw(own_key, shape, width, reach, shards=(), kind=jnp.bfloat16):
    result = width * jax.random.normal(own_key, shape, jnp.float32)
    if shards:
        result = result * block_scale(own_key, shape, shards, -0.22, 0.18)
    return jnp.clip(result, -reach, reach).astype(kind)


def noise_with(key, extent, spread, reach, cuts, heavy, held_as=jnp.bfloat16):
    array = spread * jax.random.normal(key, extent, jnp.float32)
    if cuts:
        array = array * block_scale(key, extent, cuts, -0.22, 0.18)
    return jnp.clip(with_spikes(array, jax.random.fold_in(key, 3), *heavy), -reach, reach).astype(held_as)


def setup_inputs(seed: int = 0) -> dict:
    arg_keys = jax.random.split(jax.random.key(seed), 16)
    mix_rows = bell_draw(arg_keys[0], (SEQ_LEN, D), 1.0, 6.0, ((0, 8),))
    mix_gain = jnp.clip(1.0 + 0.18 * jax.random.normal(arg_keys[1], (D,), jnp.float32), 0.099609375, 1.8984375).astype(jnp.bfloat16)
    w_query = bell_draw(arg_keys[2], (ATT, D), D ** -0.5, 0.125, ((0, 4),))
    w_key = bell_draw(arg_keys[3], (ATT, D), D ** -0.5, 0.125, ((0, 4),))
    w_value = bell_draw(arg_keys[4], (ATT, D), D ** -0.5, 0.125, ((0, 4),))
    key_offset = draw_key_offset(jax.random.fold_in(arg_keys[15], 71), 0)
    w_out = bell_draw(arg_keys[6], (ATT, D), ATT ** -0.5, 0.1875, ((0, 4),))
    out_gain = jnp.clip(1.0 + 0.18 * jax.random.normal(arg_keys[7], (D,), jnp.float32), 0.099609375, 1.8984375).astype(jnp.bfloat16)
    exp_rows = draw_exp_rows(jax.random.fold_in(arg_keys[15], 71), 0)
    exp_gain = jnp.clip(1.0 + 0.18 * jax.random.normal(arg_keys[9], (D,), jnp.float32), 0.099609375, 1.8984375).astype(jnp.bfloat16)
    routes_keys = jax.random.split(jax.random.fold_in(arg_keys[10], 1), TOK_B // EXP_ROWS)
    routes_turns = jax.random.permutation(jax.random.fold_in(arg_keys[10], 3), TOK_B // EXP_ROWS)
    routes = jax.vmap(lambda own, number: routed_block(jax.random.fold_in(arg_keys[10], 2), own, number, EXP_ROWS, EXPERTS, TOPK, CAP, 1))(routes_keys, routes_turns).reshape((TOK_B, TOPK))
    route_weight = jnp.clip(jnp.exp(math.log(1.0) - 2.9957323 * jax.random.uniform(arg_keys[11], (TOK_B, TOPK), jnp.float32) ** block_scale(arg_keys[11], (TOK_B, TOPK), ((0, 8),), -0.2, 0.2)), 0.05, 1.0)
    w_gate = draw_w_gate(jax.random.fold_in(arg_keys[15], 71), 0)
    w_up = draw_w_up(jax.random.fold_in(arg_keys[15], 71), 0)
    w_down = noise_with(arg_keys[14], (EXPERTS, FF, D), FF ** -0.5, 0.1875, ((0, 8), (1, 4)), (1, 2, 4, 2.0))
    return {"mix_rows": mix_rows, "mix_gain": mix_gain, "w_query": w_query, "w_key": w_key, "w_value": w_value, "key_offset": key_offset, "w_out": w_out, "out_gain": out_gain, "exp_rows": exp_rows, "exp_gain": exp_gain, "routes": routes, "route_weight": route_weight, "w_gate": w_gate, "w_up": w_up, "w_down": w_down}


EPSILON = 1e-06
CLAMP_LIMIT = 7.0
SILU_SHARPNESS = 1.702

def normalize(matrix, gain):
    numbers = matrix.astype(jnp.float32)
    factor = lax.rsqrt(lax.optimization_barrier(jnp.mean(numbers * numbers, axis=-1, keepdims=True)) + EPSILON)
    return numbers * factor * gain.astype(jnp.float32)

def project(normed, weight):
    product = lax.dot_general(normed, weight, (((1,), (1,)), ((), ())), preferred_element_type=jnp.float32)
    return product.astype(jnp.bfloat16)

def stick_weights(scores, visible):
    keep_log = jnp.where(visible, jax.nn.log_sigmoid(-scores), 0.0)
    later_sum = lax.cumsum(keep_log, axis=2, reverse=True) - keep_log
    return jnp.where(visible, jnp.exp(jax.nn.log_sigmoid(scores) + later_sum), 0.0)

def gated_units(gate_pre, up_pre):
    gate_part = jnp.minimum(gate_pre, CLAMP_LIMIT)
    up_part = jnp.clip(up_pre, -CLAMP_LIMIT, CLAMP_LIMIT)
    return (up_part + 1.0) * (gate_part * jax.nn.sigmoid(SILU_SHARPNESS * gate_part))

def reference(mix_rows, mix_gain, w_query, w_key, w_value, key_offset, w_out, out_gain, exp_rows, exp_gain, routes, route_weight, w_gate, w_up, w_down):
    normed = normalize(mix_rows, mix_gain).astype(jnp.bfloat16)
    length = normed.shape[0]
    queries = project(normed, w_query).astype(jnp.float32).reshape(length, ATTENTION_HEADS, HEAD)
    key_rows = project(normed, w_key).astype(jnp.float32).reshape(length, ATTENTION_HEADS, HEAD)
    value_rows = project(normed, w_value).astype(jnp.float32).reshape(length, ATTENTION_HEADS, HEAD)
    offset_values = key_offset.astype(jnp.float32)
    key_index = jnp.arange(length, dtype=jnp.int32)

    def one_block(first_row):
        block_q = lax.dynamic_slice_in_dim(queries, first_row, MIX_ROWS, 0)
        scores = jnp.einsum('thd,shd->hts', block_q, key_rows) / math.sqrt(HEAD) + offset_values[:, None, :]
        query_index = first_row + jnp.arange(MIX_ROWS, dtype=jnp.int32)
        visible = (key_index[None, :] < query_index[:, None])[None]
        weights = stick_weights(scores, visible).astype(jnp.bfloat16)
        weights = lax.optimization_barrier(weights).astype(jnp.float32)
        return jnp.einsum('hts,shd->thd', weights, value_rows)
    starts = jnp.arange(length // MIX_ROWS, dtype=jnp.int32) * MIX_ROWS
    attended = lax.map(one_block, starts).reshape(length, ATTENTION_HEADS * HEAD).astype(jnp.bfloat16)
    mixed_sum = jnp.dot(attended, w_out, preferred_element_type=jnp.float32)
    mix_out = normalize(mixed_sum, out_gain).astype(jnp.bfloat16)
    tokens = exp_rows.shape[0]
    normed_exp = normalize(exp_rows, exp_gain).astype(jnp.bfloat16)
    route_list = routes.reshape(-1).astype(jnp.int32)
    pair_count = route_list.shape[0]
    owners = jnp.arange(pair_count, dtype=jnp.int32) // TOPK
    block_of = owners // EXP_ROWS
    matches = (route_list[:, None] == jnp.arange(EXPERTS, dtype=jnp.int32)[None, :]).astype(jnp.int32)
    grouped = matches.reshape(tokens // EXP_ROWS, EXP_ROWS * TOPK, EXPERTS)
    earlier = (jnp.cumsum(grouped, axis=1) - grouped).reshape(pair_count, EXPERTS)
    slot_index = block_of * CAP + lax.optimization_barrier(jnp.sum(earlier * matches, axis=1))
    table = jnp.full((EXPERTS, tokens // EXP_ROWS * CAP), -1, jnp.int32).at[route_list, slot_index].set(owners)
    piece_count = FF // FF_PART

    def one_expert(operands):
        chosen, gate_weight, up_weight, down_weight = operands
        expert_rows = jnp.where(chosen[:, None] >= 0, normed_exp[jnp.maximum(chosen, 0)], jnp.zeros((), jnp.bfloat16))
        gate_pre = jnp.dot(expert_rows, gate_weight, preferred_element_type=jnp.float32)
        up_pre = jnp.dot(expert_rows, up_weight, preferred_element_type=jnp.float32)
        hidden = gated_units(gate_pre, up_pre).astype(jnp.bfloat16)
        row_total = hidden.shape[0]
        partials = jnp.einsum('spw,pwd->psd', hidden.astype(jnp.float32).reshape(row_total, piece_count, FF_PART), down_weight.astype(jnp.float32).reshape(piece_count, FF_PART, D))
        partials = lax.optimization_barrier(partials.astype(jnp.bfloat16)).astype(jnp.float32)
        return lax.optimization_barrier(jnp.sum(partials, axis=0)).astype(jnp.bfloat16)
    expert_out = lax.map(one_expert, (table, w_gate, w_up, w_down))
    picked = expert_out[route_list, slot_index].astype(jnp.float32).reshape(tokens, TOPK, D)
    exp_out = lax.optimization_barrier(jnp.sum(picked * route_weight.astype(jnp.float32)[:, :, None], axis=1)).astype(jnp.bfloat16)
    return (mix_out, exp_out)
```

```python
import functools
import math

import jax
import jax.numpy as jnp
from jax import lax
from jax.experimental import pallas as pl
from jax.experimental.pallas import tpu as pltpu
from jax.sharding import PartitionSpec as P

EPSILON = 1e-06
CLAMP_LIMIT = 7.0
SILU_SHARPNESS = 1.702
MESH = pl.DeviceIdType.MESH


def normalize(numbers, gain):
    factor = lax.rsqrt(jnp.mean(numbers * numbers, axis=-1, keepdims=True) + EPSILON)
    return numbers * factor * gain.astype(jnp.float32)


def project(normed, weight):
    return lax.dot_general(
        normed, weight, (((1,), (1,)), ((), ())), preferred_element_type=jnp.float32
    )


def gated_units(gate_pre, up_pre):
    gate_part = jnp.minimum(gate_pre, CLAMP_LIMIT)
    up_part = jnp.clip(up_pre, -CLAMP_LIMIT, CLAMP_LIMIT)
    return (up_part + 1.0) * (gate_part * jax.nn.sigmoid(SILU_SHARPNESS * gate_part))


def stick_block(q, kv, off, carry, acc, later, visible):
    scores = (
        lax.dot_general(q, kv, (((1,), (1,)), ((), ())), preferred_element_type=jnp.float32) + off
    )
    keep = -(jnp.maximum(scores, 0.0) + jnp.log(1.0 + jnp.exp(-jnp.abs(scores))))
    own = scores + keep
    if visible is not None:
        keep = jnp.where(visible, keep, 0.0)
    beyond = jnp.dot(keep.astype(jnp.bfloat16), later, preferred_element_type=jnp.float32)
    weights = jnp.exp(own + beyond + carry)
    if visible is not None:
        weights = jnp.where(visible, weights, 0.0)
    acc = acc + jnp.dot(weights.astype(jnp.bfloat16), kv, preferred_element_type=jnp.float32)
    return carry + jnp.sum(keep, axis=1, keepdims=True), acc


def kernel(
    dims, routes_ref, scale_ref, gains_ref, off_ref, exp_ref, mix_hbm, wq_hbm, wk_hbm, wv_hbm,
    wg_hbm, wu_hbm, wd_hbm, wo_hbm,
    out_ref, exp_out_ref,
    mix_ref, normed_ref, wq_ref, wkv_ref, kv_ref, q_ref, x_out, key_ref, weight_ref, ret_ref,
    kv_all, q_all, seg_ref, wg_ref, wu_ref, wd_ref, wo_ref, sum_ref, e_got, e_pair, e_y, e_fin,
    att_ref, att_all, att_rows, m_send, m_got, m_sum,
    kv_send, kv_recv, k_send, q_send, q_recv, x_send, x_recv, p_send, p_recv, g_send, g_recv,
    f_send, f_recv, d_send, d_recv, y_send, y_recv, z_send, z_recv, a_send, a_recv,
    h_send, h_recv, v_send, v_recv, o_send, o_recv, mix_sem, w_sem,
):
    ep, tp, share, part, packed, cap = dims
    chips = tp // 2
    heads = ep // share
    me = lax.axis_index("ep")
    mt = lax.axis_index("tp")
    core = lax.rem(mt, 2)
    partner = mt + 1 - 2 * core
    token_count, width = exp_ref.shape
    full = seg_ref.shape[1]
    head_size = wk_hbm.shape[0] // heads
    tail_rows = seg_ref.shape[0] - ep * cap
    block = kv_ref.shape[1]
    half = out_ref.shape[0] // 2
    pieces = o_send.shape[0]
    piece = half // pieces
    groups = d_send.shape[1]
    per = ep // groups

    def peer(s):
        return lax.rem(me + s, ep)

    def before(s):
        return lax.rem(me - s + ep, ep)

    def other(k):
        return lax.rem(mt + 2 * k, tp)

    stride = head_size if packed else 2 * head_size
    places = [(mix_hbm, mix_ref)]
    for h in range(heads):
        one = pl.ds(h * head_size, head_size)
        places.append((wk_hbm.at[one], wkv_ref.at[pl.ds(2 * h * head_size, head_size)]))
        places.append((wv_hbm.at[one], wkv_ref.at[pl.ds((2 * h + 1) * head_size, head_size)]))
        places.append((wq_hbm.at[one], wq_ref.at[pl.ds(h * stride, head_size)]))
    mix_loads = [
        pltpu.make_async_copy(src, dst, mix_sem.at[i]) for i, (src, dst) in enumerate(places)
    ]
    for copy in mix_loads:
        copy.start()
    weights = [
        pltpu.make_async_copy(src, dst, w_sem.at[i])
        for i, (src, dst) in enumerate(
            [(wg_hbm, wg_ref), (wu_hbm, wu_ref), (wd_hbm, wd_ref), (wo_hbm, wo_ref)]
        )
    ]
    for copy in weights:
        copy.start()

    barrier = pltpu.get_barrier_semaphore()

    def greet(s, _):
        pl.semaphore_signal(barrier, inc=1, device_id={"ep": peer(s)}, device_id_type=MESH)
        return 0

    lax.fori_loop(1, ep, greet, 0)
    pl.semaphore_signal(barrier, inc=1, device_id={"tp": partner}, device_id_type=MESH)
    for k in range(1, chips):
        pl.semaphore_signal(barrier, inc=1, device_id={"tp": other(k)}, device_id_type=MESH)

    def remote(src, dst, send, recv, where):
        return pltpu.make_async_remote_copy(
            src_ref=src, dst_ref=dst, send_sem=send, recv_sem=recv,
            device_id=where, device_id_type=MESH,
        )

    def rows(s):
        return pl.ds(s * cap, cap)

    def columns(t):
        return pl.ds(pl.multiple_of(t * width, 128), width)

    def x_copy(s):
        return remote(
            x_out.at[s], seg_ref.at[rows(s), columns(mt)], x_send.at[s], x_recv.at[s],
            {"ep": peer(s)},
        )

    def kv_copy(dest, slot):
        return remote(
            kv_ref.at[dest // share], kv_all.at[slot], kv_send.at[dest], kv_recv.at[slot],
            {"ep": dest},
        )

    def k_copy(slot):
        return remote(
            kv_all.at[slot], kv_all.at[slot], k_send.at[slot], kv_recv.at[slot], {"ep": twin}
        )

    def q_copy(dest, slot):
        return remote(
            q_ref.at[dest], q_all.at[slot], q_send.at[dest], q_recv.at[slot], {"ep": dest}
        )

    tail = pl.ds(ep * cap, tail_rows)
    step = 2 if share % 2 == 0 else 1
    twin = me + 1 - 2 * lax.rem(me, 2)

    expert_ids = lax.broadcasted_iota(jnp.int32, (ep, token_count), 0)
    chosen = jnp.zeros((ep, token_count), jnp.float32)
    weight = jnp.zeros((ep, token_count), jnp.float32)
    for k in range(routes_ref.shape[0]):
        hit = routes_ref[k : k + 1, :] == expert_ids
        chosen = jnp.where(hit, 1.0, chosen)
        weight = jnp.where(hit, scale_ref[k : k + 1, :], weight)
    earlier = (
        lax.broadcasted_iota(jnp.int32, (token_count, token_count), 0)
        < lax.broadcasted_iota(jnp.int32, (token_count, token_count), 1)
    ).astype(jnp.float32)
    slot_of = jnp.dot(chosen, earlier, preferred_element_type=jnp.float32)
    key_ref[...] = jnp.where(chosen > 0.0, slot_of, -1.0)
    weight_ref[...] = weight
    slot_ids = lax.broadcasted_iota(jnp.int32, (cap, token_count), 0).astype(jnp.float32)

    def placed(e):
        return key_ref[pl.ds(e, 1), :] == slot_ids

    def routed(s):
        picked = jnp.where(placed(peer(s)), 1.0, 0.0).astype(jnp.bfloat16)
        return jnp.dot(picked, exp_ref[...], preferred_element_type=jnp.float32).astype(
            jnp.bfloat16
        )

    for s in range(1, ep):
        x_out[s] = routed(s)
    pl.semaphore_wait(barrier, ep - 1 + 1 + chips - 1)
    for s in range(1, ep):
        x_copy(s).start()
    exp_gain = gains_ref[:, 2 * full :]
    seg_ref[tail, columns(mt)] = jnp.broadcast_to(exp_gain, (tail_rows, width)).astype(jnp.bfloat16)
    seg_ref[rows(0), columns(mt)] = routed(0)

    def rows_of(n):
        return tail if n == ep else rows(n)

    def p_copy(n):
        at = seg_ref.at[rows_of(n), columns(mt)]
        return remote(at, at, p_send.at[n], p_recv.at[n], {"tp": partner})

    def g_copy(n, k):
        at = seg_ref.at[rows_of(n), columns(mt)]
        return remote(at, at, g_send.at[k, n], g_recv.at[k, n], {"tp": other(k)})

    def f_copy(n, k):
        at = seg_ref.at[rows_of(n), columns(lax.rem(mt - 2 * k + tp, tp))]
        return remote(at, at, f_send.at[k, n], f_recv.at[k, n], {"tp": partner})

    def spread(n):
        if 0 < n < ep:
            x_copy(n).wait_recv()
        for k in range(1, chips):
            g_copy(n, k).start()
        p_copy(n).start()

    def forward(n):
        for k in range(1, chips):
            g_copy(n, k).wait_recv()
            f_copy(n, k).start()

    def gathered(n):
        p_copy(n).wait_recv()
        for k in range(1, chips):
            f_copy(n, k).wait_recv()

    def d_copy(k, g):
        at = pl.ds(g * per * cap, per * cap)
        return remote(
            sum_ref.at[at, columns(lax.rem(partner + 2 * k, tp))], e_got.at[k, at],
            d_send.at[k, g], d_recv.at[k, g], {"tp": partner},
        )

    def y_copy(k, s):
        return remote(
            e_pair.at[k - 1, rows(s)], e_y.at[k - 1, rows(s)], y_send.at[k, s],
            y_recv.at[k, s], {"tp": other(k)},
        )

    def z_copy(s):
        place = ret_ref.at[pl.ds(pl.multiple_of(me * cap, cap), cap)]
        return remote(
            e_fin.at[rows(s)], place, z_send.at[s], z_recv.at[s], {"ep": before(s)}
        )

    def z_arrived(s):
        place = ret_ref.at[pl.ds(pl.multiple_of(peer(s) * cap, cap), cap)]
        return remote(
            e_fin.at[rows(s)], place, z_send.at[s], z_recv.at[s], {"ep": before(s)}
        )

    def expert(g):
        at = pl.ds(g * per * cap, per * cap)
        gains = seg_ref[tail, :][:1]
        segment = normalize(seg_ref[at, :].astype(jnp.float32), gains).astype(jnp.bfloat16)
        gate_pre = jnp.dot(segment, wg_ref[...], preferred_element_type=jnp.float32)
        up_pre = jnp.dot(segment, wu_ref[...], preferred_element_type=jnp.float32)
        hidden = gated_units(gate_pre, up_pre).astype(jnp.bfloat16)
        sum_ref[at, :] = jnp.dot(
            hidden, wd_ref[...], preferred_element_type=jnp.float32
        ).astype(jnp.bfloat16)
        for k in list(range(1, chips)) + [0]:
            d_copy(k, g).start()

    def pair(g):
        for k in range(1, chips):
            d_copy(k, g).wait_recv()
        for s in range(g * per, (g + 1) * per):
            for k in range(1, chips):
                mine = sum_ref[rows(s), columns(other(k))].astype(jnp.float32)
                both = mine + e_got[k, rows(s), :].astype(jnp.float32)
                e_pair[k - 1, rows(s), :] = both.astype(jnp.bfloat16)
                y_copy(k, s).start()
        d_copy(0, g).wait_recv()

    early = ep // 2 - 1

    def fin(s):
        total = sum_ref[rows(s), columns(mt)].astype(jnp.float32)
        total = total + e_got[0, rows(s), :].astype(jnp.float32)
        for k in range(1, chips):
            y_copy(k, s).wait_recv()
            total = total + e_y[k - 1, rows(s), :].astype(jnp.float32)
        if s > 0:
            e_fin[rows(s), :] = total.astype(jnp.bfloat16)
        else:
            ret_ref[pl.ds(pl.multiple_of(me * cap, cap), cap), :] = total.astype(jnp.bfloat16)
        if 0 < s <= early:
            z_copy(s).start()

    spread(ep)
    spread(0)

    def send_mix():
        for copy in mix_loads:
            copy.wait()
        gain = gains_ref[:, :full]
        chunk = min(64, block)
        for r in range(0, block, chunk):
            at = pl.ds(r, chunk)
            normed_ref[at, :] = normalize(mix_ref[at, :].astype(jnp.float32), gain).astype(
                jnp.bfloat16
            )
        if not packed:
            for h in range(heads):
                at = pl.ds(h * stride + head_size, head_size)
                wq_ref[at, :] = jnp.zeros((head_size, full), jnp.bfloat16)
        both = project(normed_ref[...], wkv_ref[...])
        for h in range(heads):
            kv_ref[h] = both[:, h * 128 : (h + 1) * 128].astype(jnp.bfloat16)
        kv_all[me] = kv_ref[me // share]
        for i in range(step, ep, step):
            dest = lax.rem(me + i, ep)
            kv_copy(dest, me).start()
        if step == 2:
            k_copy(me).start()
        q = project(normed_ref[...], wq_ref[...]) * (1.0 / math.sqrt(head_size))
        for r in range(share):
            one = q[r * part : (r + 1) * part]
            if packed:
                first, second = one[: part // 2], one[part // 2 :]
                for h in range(0, heads, 2):
                    at = slice(h * head_size, (h + 2) * head_size)
                    left, right = first[:, at], second[:, at]
                    even = jnp.where(lane < 64, left, pltpu.roll(right, 64, 1))
                    odd = jnp.where(lane < 64, pltpu.roll(left, 64, 1), right)
                    q_ref[h * share + r] = even.astype(jnp.bfloat16)
                    q_ref[(h + 1) * share + r] = odd.astype(jnp.bfloat16)
            else:
                for h in range(heads):
                    q_ref[h * share + r] = one[:, h * 128 : (h + 1) * 128].astype(jnp.bfloat16)
        q_all[me] = q_ref[me]

        def send_q(s, _):
            q_copy(peer(s), me).start()
            return 0

        lax.fori_loop(1, ep, send_q, 0)

    def pass_on(i):
        slot = lax.rem(me - i + ep, ep)
        kv_copy(peer(1), slot).wait_recv()
        k_copy(slot).start()

    lane = lax.broadcasted_iota(jnp.int32, (1, 128), 1)
    send_mix()
    for n in range(1, ep):
        spread(n)
        if n == 1:
            forward(ep)
            forward(0)
        if n >= 3:
            forward(n - 2)
    if ep == 1:
        forward(ep)
        forward(0)
    for n in range(max(1, ep - 2), ep):
        forward(n)
    for g in range(groups):
        first, last = g * per, (g + 1) * per
        if g == 0:
            gathered(ep)
            for copy in weights:
                copy.wait()
        else:
            pair(g - 1)
        for s in range(first, last):
            gathered(s)
        expert(g)
    if step == 2:
        for i in range(2, ep, 2):
            pass_on(i)

    def q_wait(s, _):
        q_copy(peer(s), before(s)).wait_recv()
        return 0

    lax.fori_loop(1, ep, q_wait, 0)

    def queries(i):
        both = q_all[i].astype(jnp.float32)
        if packed:
            both = jnp.concatenate([both, pltpu.roll(both, 64, 1)], axis=0)
        return jnp.where(lane < 64, both, 0.0).astype(jnp.bfloat16)

    later = (
        lax.broadcasted_iota(jnp.int32, (block, block), 0)
        > lax.broadcasted_iota(jnp.int32, (block, block), 1)
    ).astype(jnp.float32).astype(jnp.bfloat16)
    row = lax.broadcasted_iota(jnp.int32, (part, block), 0) + lax.rem(me, share) * part
    visible = lax.broadcasted_iota(jnp.int32, (part, block), 1) < row
    carry = acc = q_rest = None
    done = 0
    for n in range(ep):
        j = ep - 1 - n

        @pl.when((me != j) if step == 1 else (lax.rem(me, 2) != j % 2))
        def _():
            kv_copy(peer(1), j).wait_recv()

        kv = kv_all[j]
        off = off_ref[pl.ds(me // share, 1), j * block : (j + 1) * block]
        q = queries(j)
        zero_carry = jnp.zeros((part, 1), jnp.float32)
        zero_acc = jnp.zeros((part, 128), jnp.float32)
        new_carry, new_acc = stick_block(q, kv, off, zero_carry, zero_acc, later, visible)
        if n == 0:
            carry, acc, q_rest = new_carry, new_acc, q
        else:
            carry, acc = stick_block(q_rest, kv, off, carry, acc, later, None)
            carry = jnp.concatenate([new_carry, carry], axis=0)
            acc = jnp.concatenate([new_acc, acc], axis=0)
            q_rest = jnp.concatenate([q, q_rest], axis=0)
        if n == min(1, ep - 1):
            pair(groups - 1)
        if n >= 1:
            fin(done)
            done = done + 1
    for i in range(ep):
        block_out = acc[i * part : (i + 1) * part]
        if packed:
            middle = part // 2
            block_out = jnp.where(
                lane < 64, pltpu.roll(block_out[:middle], 64, 1), block_out[middle:]
            )
        att_ref[i] = block_out.astype(jnp.bfloat16)

    def a_copy(dest, slot):
        return remote(
            att_ref.at[dest], att_all.at[slot], a_send.at[dest], a_recv.at[slot], {"ep": dest}
        )

    def start_a(s, _):
        a_copy(peer(s), me).start()
        return 0

    lax.fori_loop(1, ep, start_a, 0)
    att_all[me] = att_ref[me]
    for s in range(done, ep):
        fin(s)
    for s in range(early + 1, ep):
        z_copy(s).start()

    def wait_a(s, _):
        a_copy(peer(s), before(s)).wait_recv()
        return 0

    lax.fori_loop(1, ep, wait_a, 0)
    for r in range(share):
        got = [att_all[h * share + r].astype(jnp.float32) for h in range(heads)]
        if packed:
            upper = []
            lower = []
            for h in range(0, heads, 2):
                upper.append(jnp.where(lane < 64, got[h], pltpu.roll(got[h + 1], 64, 1)))
                lower.append(jnp.where(lane < 64, pltpu.roll(got[h], 64, 1), got[h + 1]))
            both = jnp.concatenate(
                [jnp.concatenate(upper, axis=1), jnp.concatenate(lower, axis=1)], axis=0
            )
        else:
            both = []
            for h in range(heads):
                both.append(jnp.where(lane < 64, 0.0, got[h]))
            both = jnp.concatenate(both, axis=1)
        att_rows[pl.ds(r * part, part), :] = both.astype(jnp.bfloat16)

    def half_rows(c):
        return pl.ds(pl.multiple_of(c * half, half), half)

    h_copy = remote(m_send, m_got, h_send.at[0], h_recv.at[0], {"tp": partner})
    m_send[...] = jnp.dot(
        att_rows[half_rows(1 - core), :], wo_ref[...], preferred_element_type=jnp.float32
    ).astype(jnp.bfloat16)
    h_copy.start()
    mine = jnp.dot(att_rows[half_rows(core), :], wo_ref[...], preferred_element_type=jnp.float32)
    h_copy.wait_recv()

    def v_copy(k, i):
        at = pl.ds(i * piece, piece)
        return remote(
            m_sum.at[0, at], m_sum.at[k, at], v_send.at[k, i], v_recv.at[k, i],
            {"tp": other(k)},
        )

    for i in range(pieces):
        at = pl.ds(i * piece, piece)
        pair = mine[i * piece : (i + 1) * piece] + m_got[at, :].astype(jnp.float32)
        m_sum[0, at, :] = pair.astype(jnp.bfloat16)
        for k in range(1, chips):
            v_copy(k, i).start()

    def o_copy(i):
        at = out_ref.at[pl.ds(pl.multiple_of(core * half + i * piece, piece), piece)]
        return remote(at, at, o_send.at[i], o_recv.at[i], {"tp": partner})

    gain = gains_ref[:, full : 2 * full]

    def combine():
        total = jnp.zeros((token_count, width), jnp.float32)
        for s in range(ep):
            if s > 0:
                z_arrived(s).wait_recv()
            e = peer(s)
            spread_to = jnp.where(placed(e), weight_ref[pl.ds(e, 1), :], 0.0)
            high = spread_to.astype(jnp.bfloat16).astype(jnp.float32)
            both = jnp.concatenate([high, spread_to - high], axis=0).T.astype(jnp.bfloat16)
            got = ret_ref[pl.ds(pl.multiple_of(e * cap, cap), cap), :]
            for low in range(2):
                total = total + jnp.dot(
                    both[:, low * cap : (low + 1) * cap], got, preferred_element_type=jnp.float32
                )
        exp_out_ref[...] = total.astype(jnp.bfloat16)

    for i in range(pieces):
        at = pl.ds(i * piece, piece)
        if i == min(2, pieces - 1):
            combine()
        for k in range(1, chips):
            v_copy(k, i).wait_recv()
        total = jnp.zeros((piece, out_ref.shape[1]), jnp.float32)
        for chip in range(chips):
            slot = lax.rem(mt // 2 - chip + chips, chips)
            total = total + m_sum[slot, at, :].astype(jnp.float32)
        own_rows = pl.ds(pl.multiple_of(core * half + i * piece, piece), piece)
        out_ref[own_rows, :] = normalize(total, gain).astype(jnp.bfloat16)
        o_copy(i).start()

    h_copy.wait_send()
    for n in range(ep + 1):
        p_copy(n).wait_send()
        for k in range(1, chips):
            g_copy(n, k).wait_send()
            f_copy(n, k).wait_send()
    for k in range(chips):
        for g in range(groups):
            d_copy(k, g).wait_send()
    for k in range(1, chips):
        for s in range(ep):
            y_copy(k, s).wait_send()
        for i in range(pieces):
            v_copy(k, i).wait_send()
    for s in range(1, ep):
        x_copy(s).wait_send()
        z_copy(s).wait_send()

    def finish(s, _):
        q_copy(peer(s), me).wait_send()
        a_copy(peer(s), me).wait_send()
        return 0

    lax.fori_loop(1, ep, finish, 0)
    for i in range(step, ep, step):
        kv_copy(lax.rem(me + i, ep), me).wait_send()
    if step == 2:
        for i in range(0, ep, 2):
            k_copy(lax.rem(me - i + ep, ep)).wait_send()
    for i in range(pieces):
        at = out_ref.at[pl.ds(pl.multiple_of((1 - core) * half + i * piece, piece), piece)]
        remote(at, at, o_send.at[i], o_recv.at[i], {"tp": partner}).wait_recv()
        o_copy(i).wait_send()


def one_call(
    ep, tp, share, part, packed, cap, routes, scale, gains, off, exp_rows, mix, wq, wk, wv,
    wg, wu, wd, wo,
):
    token_count, width = exp_rows.shape
    row_count, full = mix.shape
    heads = off.shape[0]
    head_size = wq.shape[0] // heads
    slots = ep * cap
    chips = tp // 2
    half = row_count // 2
    pieces = 4
    groups = 2 if ep % 2 == 0 else 1
    others = max(chips - 1, 1)
    q_rows = part // 2 if packed else part
    q_stride = head_size if packed else 2 * head_size
    dma = pltpu.SemaphoreType.DMA
    vmem = pl.BlockSpec(memory_space=pltpu.VMEM)
    hbm = pl.BlockSpec(memory_space=pl.ANY)

    def held(*shape):
        return pltpu.VMEM(shape, jnp.bfloat16)

    def both(*shape):
        return [dma(shape), dma(shape)]

    return pl.pallas_call(
        functools.partial(kernel, (ep, tp, share, part, packed, cap)),
        out_shape=(
            jax.ShapeDtypeStruct((row_count, full), jnp.bfloat16),
            jax.ShapeDtypeStruct((token_count, width), jnp.bfloat16),
        ),
        in_specs=[vmem] * 5 + [hbm] * 8,
        out_specs=(vmem, vmem),
        scratch_shapes=[
            held(row_count, full), held(row_count, full), held(heads * q_stride, full),
            held(2 * heads * head_size, full), held(heads, row_count, 128),
            held(ep, q_rows, 128), held(ep, cap, width),
            pltpu.VMEM((ep, token_count), jnp.float32), pltpu.VMEM((ep, token_count), jnp.float32),
            held(slots, width),
            held(ep, row_count, 128), held(ep, q_rows, 128),
            held(slots + 16, full),
            held(*wg.shape), held(*wu.shape), held(*wd.shape), held(*wo.shape),
            held(slots, full), held(chips, slots, width), held(others, slots, width),
            held(others, slots, width), held(slots, width),
            held(ep, q_rows, 128), held(ep, q_rows, 128), held(row_count, wo.shape[0]),
            held(half, full), held(half, full), held(chips, half, full),
        ]
        + both(ep) + [dma((ep,))] + both(ep) + both(ep) + both(ep + 1) + both(chips, ep + 1)
        + both(chips, ep + 1) + both(chips, groups) + both(chips, ep) + both(ep) + both(ep)
        + both(1) + both(chips, pieces) + both(pieces) + [dma((1 + 3 * heads,)), dma((4,))],
        compiler_params=pltpu.CompilerParams(
            collective_id=0, has_side_effects=True, vmem_limit_bytes=60 * 1024 * 1024
        ),
    )(routes, scale, gains, off, exp_rows, mix, wq, wk, wv, wg, wu, wd, wo)


def on_device(
    mix_rows,
    mix_gain,
    w_query,
    w_key,
    w_value,
    key_offset,
    w_out,
    out_gain,
    exp_rows,
    exp_gain,
    routes,
    route_weight,
    w_gate,
    w_up,
    w_down,
):
    ep = lax.axis_size("ep")
    tp = lax.axis_size("tp")
    row_count = mix_rows.shape[0]
    heads_here = key_offset.shape[0]
    head_size = w_query.shape[0] // heads_here
    share = ep // heads_here
    part = row_count // share
    packed = part % 32 == 0 and heads_here % 2 == 0
    token_count, top_count = routes.shape
    experts = w_gate.shape[0] * ep
    capacity = 4 * token_count * top_count // (3 * experts)
    gains = jnp.concatenate([mix_gain, out_gain, exp_gain]).astype(jnp.float32)[None]
    if not packed:
        w_out = w_out.reshape(heads_here, head_size, -1)
        w_out = jnp.concatenate([jnp.zeros_like(w_out), w_out], axis=1)
        w_out = w_out.reshape(2 * heads_here * head_size, -1)
    mix_out, exp_out = one_call(
        ep, tp, share, part, packed, capacity, routes.T, route_weight.T, gains, key_offset,
        exp_rows, mix_rows, w_query, w_key, w_value, w_gate[0], w_up[0], w_down[0], w_out,
    )
    return (mix_out, exp_out)


def solution(mesh):
    placed = (
        P("ep", None),
        P(),
        P("tp", None),
        P("tp", None),
        P("tp", None),
        P("tp", None),
        P("tp", None),
        P(),
        P("ep", "tp"),
        P("tp"),
        P("ep", None),
        P("ep", None),
        P("ep", None, "tp"),
        P("ep", None, "tp"),
        P("ep", "tp", None),
    )
    return jax.shard_map(
        on_device,
        mesh=mesh,
        in_specs=placed,
        out_specs=(P("ep", None), P("ep", "tp")),
        check_vma=False,
    )
```

```python
import functools
import math

import jax
import jax.numpy as jnp
from jax import lax
from jax.experimental import pallas as pl
from jax.experimental.pallas import tpu as pltpu
from jax.sharding import PartitionSpec as P

EPSILON = 1e-06
CLAMP_LIMIT = 7.0
SILU_SHARPNESS = 1.702
MESH = pl.DeviceIdType.MESH


def normalize(numbers, gain):
    factor = lax.rsqrt(jnp.mean(numbers * numbers, axis=-1, keepdims=True) + EPSILON)
    return numbers * factor * gain.astype(jnp.float32)


def project(normed, weight):
    return lax.dot_general(
        normed, weight, (((1,), (1,)), ((), ())), preferred_element_type=jnp.float32
    )


def gated_units(gate_pre, up_pre):
    gate_part = jnp.minimum(gate_pre, CLAMP_LIMIT)
    up_part = jnp.clip(up_pre, -CLAMP_LIMIT, CLAMP_LIMIT)
    return (up_part + 1.0) * (gate_part * jax.nn.sigmoid(SILU_SHARPNESS * gate_part))


def stick_block(q, kv, off, carry, acc, later, visible):
    scores = (
        lax.dot_general(q, kv, (((1,), (1,)), ((), ())), preferred_element_type=jnp.float32) + off
    )
    keep = -(jnp.maximum(scores, 0.0) + jnp.log(1.0 + jnp.exp(-jnp.abs(scores))))
    own = scores + keep
    if visible is not None:
        keep = jnp.where(visible, keep, 0.0)
    beyond = jnp.dot(keep.astype(jnp.bfloat16), later, preferred_element_type=jnp.float32)
    weights = jnp.exp(own + beyond + carry)
    if visible is not None:
        weights = jnp.where(visible, weights, 0.0)
    acc = acc + jnp.dot(weights.astype(jnp.bfloat16), kv, preferred_element_type=jnp.float32)
    return carry + jnp.sum(keep, axis=1, keepdims=True), acc


def kernel(
    dims, routes_ref, scale_ref, gains_ref, off_ref, exp_ref, mix_hbm, wq_hbm, wk_hbm, wv_hbm,
    wg_hbm, wu_hbm, wd_hbm, wo_hbm,
    out_ref, exp_out_ref,
    mix_ref, normed_ref, wq_ref, wkv_ref, kv_ref, q_ref, x_out, key_ref, weight_ref, ret_ref,
    kv_all, q_all, seg_ref, wg_ref, wu_ref, wd_ref, wo_ref, sum_ref, e_got, e_pair, e_y, e_fin,
    att_ref, att_all, att_rows, m_send, m_got, m_sum, att_wide,
    kv_send, kv_recv, k_send, q_send, q_recv, x_send, x_recv, p_send, p_recv, g_send, g_recv,
    f_send, f_recv, d_send, d_recv, y_send, y_recv, z_send, z_recv, a_send, a_recv,
    h_send, h_recv, v_send, v_recv, o_send, o_recv, b_send, b_recv, wy_send, wy_recv,
    wx_send, wx_recv, wd_send, wd_recv, mix_sem, w_sem,
):
    ep, tp, share, part, packed, cap = dims
    chips = tp // 2
    heads = ep // share
    me = lax.axis_index("ep")
    mt = lax.axis_index("tp")
    core = lax.rem(mt, 2)
    partner = mt + 1 - 2 * core
    token_count, width = exp_ref.shape
    full = seg_ref.shape[1]
    head_size = wk_hbm.shape[0] // heads
    tail_rows = seg_ref.shape[0] - ep * cap
    block = kv_ref.shape[1]
    half = out_ref.shape[0] // 2
    pieces = o_send.shape[0]
    piece = half // pieces
    groups = d_send.shape[1]
    per = ep // groups
    channels = wo_hbm.shape[0]
    wide = wo_ref.shape[0] > channels
    mine_at = pl.multiple_of(mt * channels, 128) if wide else 0
    w_pieces = wy_send.shape[0]
    w_rows = channels // 2 // w_pieces

    def peer(s):
        return lax.rem(me + s, ep)

    def before(s):
        return lax.rem(me - s + ep, ep)

    def other(k):
        return lax.rem(mt + 2 * k, tp)

    stride = head_size if packed else 2 * head_size
    places = [(mix_hbm, mix_ref)]
    for h in range(heads):
        one = pl.ds(h * head_size, head_size)
        places.append((wk_hbm.at[one], wkv_ref.at[pl.ds(2 * h * head_size, head_size)]))
        places.append((wv_hbm.at[one], wkv_ref.at[pl.ds((2 * h + 1) * head_size, head_size)]))
        places.append((wq_hbm.at[one], wq_ref.at[pl.ds(h * stride, head_size)]))
    mix_loads = [
        pltpu.make_async_copy(src, dst, mix_sem.at[i]) for i, (src, dst) in enumerate(places)
    ]
    for copy in mix_loads:
        copy.start()
    wo_place = wo_ref.at[pl.ds(mine_at, channels)]
    weights = [
        pltpu.make_async_copy(src, dst, w_sem.at[i])
        for i, (src, dst) in enumerate(
            [(wo_hbm, wo_place), (wg_hbm, wg_ref), (wu_hbm, wu_ref), (wd_hbm, wd_ref)]
        )
    ]
    for copy in weights:
        copy.start()

    barrier = pltpu.get_barrier_semaphore()

    def greet(s, _):
        pl.semaphore_signal(barrier, inc=1, device_id={"ep": peer(s)}, device_id_type=MESH)
        return 0

    lax.fori_loop(1, ep, greet, 0)
    pl.semaphore_signal(barrier, inc=1, device_id={"tp": partner}, device_id_type=MESH)
    for k in range(1, chips):
        pl.semaphore_signal(barrier, inc=1, device_id={"tp": other(k)}, device_id_type=MESH)

    def remote(src, dst, send, recv, where):
        return pltpu.make_async_remote_copy(
            src_ref=src, dst_ref=dst, send_sem=send, recv_sem=recv,
            device_id=where, device_id_type=MESH,
        )

    def rows(s):
        return pl.ds(s * cap, cap)

    def columns(t):
        return pl.ds(pl.multiple_of(t * width, 128), width)

    def x_copy(s):
        return remote(
            x_out.at[s], seg_ref.at[rows(s), columns(mt)], x_send.at[s], x_recv.at[s],
            {"ep": peer(s)},
        )

    def kv_copy(dest, slot):
        return remote(
            kv_ref.at[dest // share], kv_all.at[slot], kv_send.at[dest], kv_recv.at[slot],
            {"ep": dest},
        )

    def k_copy(slot):
        return remote(
            kv_all.at[slot], kv_all.at[slot], k_send.at[slot], kv_recv.at[slot], {"ep": twin}
        )

    def q_copy(dest, slot):
        return remote(
            q_ref.at[dest], q_all.at[slot], q_send.at[dest], q_recv.at[slot], {"ep": dest}
        )

    def w_part(t, half_of, i):
        at = pl.multiple_of(t * channels + half_of * (channels // 2) + i * w_rows, 16)
        return wo_ref.at[pl.ds(at, w_rows)]

    def w_half(t, half_of):
        at = pl.multiple_of(t * channels + half_of * (channels // 2), 16)
        return wo_ref.at[pl.ds(at, channels // 2)]

    parity = lax.rem(me, 2)

    def wy_copy(i):
        at = w_part(mt, parity, i)
        return remote(at, at, wy_send.at[i], wy_recv.at[i], {"tp": other(1)})

    def wx_copy(i):
        at = w_part(other(1), parity, i)
        return remote(at, at, wx_send.at[i], wx_recv.at[i], {"ep": twin})

    def wd_copy(i):
        at = w_half(mt if i < 2 else other(1), i if i < 2 else (parity if i == 2 else 1 - parity))
        return remote(at, at, wd_send.at[i], wd_recv.at[i], {"tp": partner})

    def w_across():
        for i in range(w_pieces):
            wy_copy(i).wait_recv()
            wx_copy(i).start()
        wd_copy(2).start()

    def w_along():
        for i in range(w_pieces):
            wx_copy(i).wait_recv()
        wd_copy(3).start()

    tail = pl.ds(ep * cap, tail_rows)
    step = 2 if share % 2 == 0 else 1
    twin = me + 1 - 2 * lax.rem(me, 2)

    def w_start(first, last):
        for i in range(first, last):
            wy_copy(i).start()

    weights[0].wait()
    pl.semaphore_wait(barrier, ep - 1 + 1 + chips - 1)
    if wide:
        w_start(0, w_pieces)
        for i in range(2):
            wd_copy(i).start()

    expert_ids = lax.broadcasted_iota(jnp.int32, (ep, token_count), 0)
    chosen = jnp.zeros((ep, token_count), jnp.float32)
    weight = jnp.zeros((ep, token_count), jnp.float32)
    for k in range(routes_ref.shape[0]):
        hit = routes_ref[k : k + 1, :] == expert_ids
        chosen = jnp.where(hit, 1.0, chosen)
        weight = jnp.where(hit, scale_ref[k : k + 1, :], weight)
    earlier = (
        lax.broadcasted_iota(jnp.int32, (token_count, token_count), 0)
        < lax.broadcasted_iota(jnp.int32, (token_count, token_count), 1)
    ).astype(jnp.float32)
    slot_of = jnp.dot(chosen, earlier, preferred_element_type=jnp.float32)
    key_ref[...] = jnp.where(chosen > 0.0, slot_of, -1.0)
    weight_ref[...] = weight
    slot_ids = lax.broadcasted_iota(jnp.int32, (cap, token_count), 0).astype(jnp.float32)

    def placed(e):
        return key_ref[pl.ds(e, 1), :] == slot_ids

    def routed(s):
        picked = jnp.where(placed(peer(s)), 1.0, 0.0).astype(jnp.bfloat16)
        return jnp.dot(picked, exp_ref[...], preferred_element_type=jnp.float32).astype(
            jnp.bfloat16
        )

    exp_gain = gains_ref[:, 2 * full :]
    seg_ref[tail, columns(mt)] = jnp.broadcast_to(exp_gain, (tail_rows, width)).astype(jnp.bfloat16)
    ahead = 3 if ep == 8 else ep

    def send_x(first, last):
        for s in range(first, last):
            x_out[s] = routed(s)
            x_copy(s).start()

    send_x(1, ahead)
    seg_ref[rows(0), columns(mt)] = routed(0)

    def rows_of(n):
        return tail if n == ep else rows(n)

    def p_copy(n):
        at = seg_ref.at[rows_of(n), columns(mt)]
        return remote(at, at, p_send.at[n], p_recv.at[n], {"tp": partner})

    def g_copy(n, k):
        at = seg_ref.at[rows_of(n), columns(mt)]
        return remote(at, at, g_send.at[k, n], g_recv.at[k, n], {"tp": other(k)})

    def f_copy(n, k):
        at = seg_ref.at[rows_of(n), columns(lax.rem(mt - 2 * k + tp, tp))]
        return remote(at, at, f_send.at[k, n], f_recv.at[k, n], {"tp": partner})

    def spread(n):
        if 0 < n < ep:
            x_copy(n).wait_recv()
        for k in range(1, chips):
            g_copy(n, k).start()
        p_copy(n).start()

    def forward(n):
        for k in range(1, chips):
            g_copy(n, k).wait_recv()
            f_copy(n, k).start()

    def gathered(n):
        p_copy(n).wait_recv()
        for k in range(1, chips):
            f_copy(n, k).wait_recv()

    def d_copy(k, g):
        at = pl.ds(g * per * cap, per * cap)
        return remote(
            sum_ref.at[at, columns(lax.rem(partner + 2 * k, tp))], e_got.at[k, at],
            d_send.at[k, g], d_recv.at[k, g], {"tp": partner},
        )

    def y_copy(k, s):
        return remote(
            e_pair.at[k - 1, rows(s)], e_y.at[k - 1, rows(s)], y_send.at[k, s],
            y_recv.at[k, s], {"tp": other(k)},
        )

    def z_copy(s):
        place = ret_ref.at[pl.ds(pl.multiple_of(me * cap, cap), cap)]
        return remote(
            e_fin.at[rows(s)], place, z_send.at[s], z_recv.at[s], {"ep": before(s)}
        )

    def z_arrived(s):
        place = ret_ref.at[pl.ds(pl.multiple_of(peer(s) * cap, cap), cap)]
        return remote(
            e_fin.at[rows(s)], place, z_send.at[s], z_recv.at[s], {"ep": before(s)}
        )

    def expert(g):
        at = pl.ds(g * per * cap, per * cap)
        gains = seg_ref[tail, :][:1]
        segment = normalize(seg_ref[at, :].astype(jnp.float32), gains).astype(jnp.bfloat16)
        gate_pre = jnp.dot(segment, wg_ref[...], preferred_element_type=jnp.float32)
        up_pre = jnp.dot(segment, wu_ref[...], preferred_element_type=jnp.float32)
        hidden = gated_units(gate_pre, up_pre).astype(jnp.bfloat16)
        sum_ref[at, :] = jnp.dot(
            hidden, wd_ref[...], preferred_element_type=jnp.float32
        ).astype(jnp.bfloat16)
        for k in list(range(1, chips)) + [0]:
            d_copy(k, g).start()

    def pair(g):
        for k in range(1, chips):
            d_copy(k, g).wait_recv()
        for s in range(g * per, (g + 1) * per):
            for k in range(1, chips):
                mine = sum_ref[rows(s), columns(other(k))].astype(jnp.float32)
                both = mine + e_got[k, rows(s), :].astype(jnp.float32)
                e_pair[k - 1, rows(s), :] = both.astype(jnp.bfloat16)
                y_copy(k, s).start()
        d_copy(0, g).wait_recv()

    early = ep - 1

    def fin(s):
        total = sum_ref[rows(s), columns(mt)].astype(jnp.float32)
        total = total + e_got[0, rows(s), :].astype(jnp.float32)
        for k in range(1, chips):
            y_copy(k, s).wait_recv()
            total = total + e_y[k - 1, rows(s), :].astype(jnp.float32)
        if s > 0:
            e_fin[rows(s), :] = total.astype(jnp.bfloat16)
        else:
            ret_ref[pl.ds(pl.multiple_of(me * cap, cap), cap), :] = total.astype(jnp.bfloat16)
        if 0 < s <= early:
            z_copy(s).start()

    def make_mix():
        for copy in mix_loads:
            copy.wait()
        gain = gains_ref[:, :full]
        chunk = min(64, block)
        for r in range(0, block, chunk):
            at = pl.ds(r, chunk)
            normed_ref[at, :] = normalize(mix_ref[at, :].astype(jnp.float32), gain).astype(
                jnp.bfloat16
            )
        if not packed:
            for h in range(heads):
                at = pl.ds(h * stride + head_size, head_size)
                wq_ref[at, :] = jnp.zeros((head_size, full), jnp.bfloat16)
        both = project(normed_ref[...], wkv_ref[...])
        for h in range(heads):
            kv_ref[h] = both[:, h * 128 : (h + 1) * 128].astype(jnp.bfloat16)
        kv_all[me] = kv_ref[me // share]
        for i in range(step, ep, step):
            kv_copy(lax.rem(me + i, ep), me).start()
        if step == 2:
            k_copy(me).start()
        q = project(normed_ref[...], wq_ref[...]) * (1.0 / math.sqrt(head_size))
        for r in range(share):
            one = q[r * part : (r + 1) * part]
            if packed:
                first, second = one[: part // 2], one[part // 2 :]
                for h in range(0, heads, 2):
                    at = slice(h * head_size, (h + 2) * head_size)
                    left, right = first[:, at], second[:, at]
                    even = jnp.where(lane < 64, left, pltpu.roll(right, 64, 1))
                    odd = jnp.where(lane < 64, pltpu.roll(left, 64, 1), right)
                    q_ref[h * share + r] = even.astype(jnp.bfloat16)
                    q_ref[(h + 1) * share + r] = odd.astype(jnp.bfloat16)
            else:
                for h in range(heads):
                    q_ref[h * share + r] = one[:, h * 128 : (h + 1) * 128].astype(jnp.bfloat16)
        q_all[me] = q_ref[me]

    def pass_on(i):
        slot = lax.rem(me - i + ep, ep)
        kv_copy(peer(1), slot).wait_recv()
        k_copy(slot).start()

    lane = lax.broadcasted_iota(jnp.int32, (1, 128), 1)
    spread(ep)
    spread(0)
    make_mix()

    def send_q(s, _):
        q_copy(peer(s), me).start()
        return 0

    lax.fori_loop(1, ep, send_q, 0)

    def kv_forward():
        if step == 2:
            for i in range(2, ep, 2):
                pass_on(i)

    def collect(g):
        if g == 0:
            gathered(ep)
            for copy in weights[1:]:
                copy.wait()
        for s in range(g * per, (g + 1) * per):
            gathered(s)

    def q_wait(s, _):
        q_copy(peer(s), before(s)).wait_recv()
        return 0

    def run_expert(g):
        collect(g)
        expert(g)

    def first_forward():
        forward(ep)
        forward(0)

    def fins(g):
        for s in range(g * per, (g + 1) * per):
            fin(s)

    tasks = []

    def add(when, act, *args):
        tasks.append((when, functools.partial(act, *args)))

    if ep == 8:
        add(-1, spread, 1)
        add(-1, spread, 2)
        add(-1, kv_forward)
        add(-1, send_x, ahead, ep)
        if wide:
            add(-1, w_across)
        add(0, first_forward)
        add(1, spread, 3)
        add(1, forward, 1)
        add(2, forward, 2)
        add(2, spread, 4)
        add(3, forward, 3)
        add(4, spread, 5)
        add(5, forward, 4)
        add(6, spread, 6)
        add(7, spread, 7)
        add(7, forward, 5)
        add(8, run_expert, 0)
        add(8, forward, 6)
        add(8, forward, 7)
        add(8, pair, 0)
        add(8, run_expert, 1)
        add(9, pair, 1)
        add(9, fins, 0)
        if wide:
            add(9, w_along)
    else:
        add(-1, kv_forward)
        for n in range(1, ep):
            add(ep, spread, n)
        add(ep, first_forward)
        for n in range(1, ep):
            add(ep, forward, n)
        for g in range(groups):
            add(ep, run_expert, g)
            if g > 0:
                add(ep, pair, g - 1)
        if wide:
            add(ep, w_across)
            add(ep, w_along)
        for g in range(groups - 1):
            add(ep, fins, g)

    for when, act in tasks:
        if when < 0:
            act()
    lax.fori_loop(1, ep, q_wait, 0)

    def queries(i):
        both = q_all[i].astype(jnp.float32)
        if packed:
            both = jnp.concatenate([both, pltpu.roll(both, 64, 1)], axis=0)
        return jnp.where(lane < 64, both, 0.0).astype(jnp.bfloat16)

    later = (
        lax.broadcasted_iota(jnp.int32, (block, block), 0)
        > lax.broadcasted_iota(jnp.int32, (block, block), 1)
    ).astype(jnp.float32).astype(jnp.bfloat16)
    row = lax.broadcasted_iota(jnp.int32, (part, block), 0) + lax.rem(me, share) * part
    visible = lax.broadcasted_iota(jnp.int32, (part, block), 1) < row
    carry = acc = q_rest = None
    for n in range(ep):
        j = ep - 1 - n

        @pl.when((me != j) if step == 1 else (lax.rem(me, 2) != j % 2))
        def _():
            kv_copy(peer(1), j).wait_recv()

        kv = kv_all[j]
        off = off_ref[pl.ds(me // share, 1), j * block : (j + 1) * block]
        q = queries(j)
        zero_carry = jnp.zeros((part, 1), jnp.float32)
        zero_acc = jnp.zeros((part, 128), jnp.float32)
        new_carry, new_acc = stick_block(q, kv, off, zero_carry, zero_acc, later, visible)
        if n == 0:
            carry, acc, q_rest = new_carry, new_acc, q
        else:
            carry, acc = stick_block(q_rest, kv, off, carry, acc, later, None)
            carry = jnp.concatenate([new_carry, carry], axis=0)
            acc = jnp.concatenate([new_acc, acc], axis=0)
            q_rest = jnp.concatenate([q, q_rest], axis=0)
        for when, act in tasks:
            if when == n:
                act()
    for i in range(ep):
        block_out = acc[i * part : (i + 1) * part]
        if packed:
            middle = part // 2
            block_out = jnp.where(
                lane < 64, pltpu.roll(block_out[:middle], 64, 1), block_out[middle:]
            )
        att_ref[i] = block_out.astype(jnp.bfloat16)

    def a_copy(dest, slot):
        return remote(
            att_ref.at[dest], att_all.at[slot], a_send.at[dest], a_recv.at[slot], {"ep": dest}
        )

    def start_a(s, _):
        a_copy(peer(s), me).start()
        return 0

    lax.fori_loop(1, ep, start_a, 0)
    att_all[me] = att_ref[me]
    for when, act in tasks:
        if when == ep:
            act()

    def wait_a(s, _):
        a_copy(peer(s), before(s)).wait_recv()
        return 0

    lax.fori_loop(1, ep, wait_a, 0)
    late = groups - 1
    for r in range(share):
        got = [att_all[h * share + r].astype(jnp.float32) for h in range(heads)]
        if packed:
            upper = []
            lower = []
            for h in range(0, heads, 2):
                upper.append(jnp.where(lane < 64, got[h], pltpu.roll(got[h + 1], 64, 1)))
                lower.append(jnp.where(lane < 64, pltpu.roll(got[h], 64, 1), got[h + 1]))
            both = jnp.concatenate(
                [jnp.concatenate(upper, axis=1), jnp.concatenate(lower, axis=1)], axis=0
            )
        else:
            both = []
            for h in range(heads):
                both.append(jnp.where(lane < 64, 0.0, got[h]))
            both = jnp.concatenate(both, axis=1)
        att_rows[pl.ds(r * part, part), :] = both.astype(jnp.bfloat16)

    def half_rows(c):
        return pl.ds(pl.multiple_of(c * half, half), half)

    def o_copy(i):
        at = out_ref.at[pl.ds(pl.multiple_of(core * half + i * piece, piece), piece)]
        return remote(at, at, o_send.at[i], o_recv.at[i], {"tp": partner})

    gain = gains_ref[:, full : 2 * full]

    def combine():
        total = jnp.zeros((token_count, width), jnp.float32)
        for s in range(ep):
            if s > 0:
                z_arrived(s).wait_recv()
            e = peer(s)
            spread_to = jnp.where(placed(e), weight_ref[pl.ds(e, 1), :], 0.0)
            high = spread_to.astype(jnp.bfloat16).astype(jnp.float32)
            both = jnp.concatenate([high, spread_to - high], axis=0).T.astype(jnp.bfloat16)
            got = ret_ref[pl.ds(pl.multiple_of(e * cap, cap), cap), :]
            for low in range(2):
                total = total + jnp.dot(
                    both[:, low * cap : (low + 1) * cap], got, preferred_element_type=jnp.float32
                )
        exp_out_ref[...] = total.astype(jnp.bfloat16)

    def b_copy(j):
        dest = lax.rem(mt + j, tp)
        return remote(
            att_rows.at[half_rows(lax.rem(dest, 2))],
            att_wide.at[:, pl.ds(mine_at, channels)],
            b_send.at[j], b_recv.at[j], {"tp": dest},
        )

    def h_copy():
        return remote(m_send, m_got, h_send.at[0], h_recv.at[0], {"tp": partner})

    def v_copy(k, i):
        at = pl.ds(i * piece, piece)
        return remote(
            m_sum.at[0, at], m_sum.at[k, at], v_send.at[k, i], v_recv.at[k, i],
            {"tp": other(k)},
        )

    def publish(i, total):
        own_rows = pl.ds(pl.multiple_of(core * half + i * piece, piece), piece)
        out_ref[own_rows, :] = normalize(total, gain).astype(jnp.bfloat16)
        o_copy(i).start()

    if wide:
        for j in range(1, tp):
            b_copy(j).start()
        att_wide[:, pl.ds(mine_at, channels)] = att_rows[half_rows(core), :]
        for when, act in tasks:
            if when == ep + 1:
                act()
        for i in range(4):
            wd_copy(i).wait_recv()
        for j in range(1, tp):
            b_copy(j).wait_recv()
        for i in range(pieces):
            total = jnp.dot(
                att_wide[i * piece : (i + 1) * piece, :], wo_ref[...],
                preferred_element_type=jnp.float32,
            )
            publish(i, total)
        fins(late)
        for s in range(early + 1, ep):
            z_copy(s).start()
        combine()
    else:
        pair(late)
        fins(late)
        for s in range(early + 1, ep):
            z_copy(s).start()
        m_send[...] = jnp.dot(
            att_rows[half_rows(1 - core), :], wo_ref[...], preferred_element_type=jnp.float32
        ).astype(jnp.bfloat16)
        h_copy().start()
        mine = jnp.dot(
            att_rows[half_rows(core), :], wo_ref[...], preferred_element_type=jnp.float32
        )
        h_copy().wait_recv()
        for i in range(pieces):
            at = pl.ds(i * piece, piece)
            both = mine[i * piece : (i + 1) * piece] + m_got[at, :].astype(jnp.float32)
            m_sum[0, at, :] = both.astype(jnp.bfloat16)
            for k in range(1, chips):
                v_copy(k, i).start()
        combine()
        for i in range(pieces):
            at = pl.ds(i * piece, piece)
            for k in range(1, chips):
                v_copy(k, i).wait_recv()
            total = jnp.zeros((piece, out_ref.shape[1]), jnp.float32)
            for chip in range(chips):
                slot = lax.rem(mt // 2 - chip + chips, chips)
                total = total + m_sum[slot, at, :].astype(jnp.float32)
            publish(i, total)

    if wide:
        for j in range(1, tp):
            b_copy(j).wait_send()
        for i in range(w_pieces):
            wy_copy(i).wait_send()
            wx_copy(i).wait_send()
        for i in range(4):
            wd_copy(i).wait_send()
    else:
        h_copy().wait_send()
        for k in range(1, chips):
            for i in range(pieces):
                v_copy(k, i).wait_send()
    for n in range(ep + 1):
        p_copy(n).wait_send()
        for k in range(1, chips):
            g_copy(n, k).wait_send()
            f_copy(n, k).wait_send()
    for k in range(chips):
        for g in range(groups):
            d_copy(k, g).wait_send()
    for k in range(1, chips):
        for s in range(ep):
            y_copy(k, s).wait_send()
    for s in range(1, ep):
        x_copy(s).wait_send()
        z_copy(s).wait_send()

    def finish(s, _):
        q_copy(peer(s), me).wait_send()
        a_copy(peer(s), me).wait_send()
        return 0

    lax.fori_loop(1, ep, finish, 0)
    for i in range(step, ep, step):
        kv_copy(lax.rem(me + i, ep), me).wait_send()
    if step == 2:
        for i in range(0, ep, 2):
            k_copy(lax.rem(me - i + ep, ep)).wait_send()
    for i in range(pieces):
        at = out_ref.at[pl.ds(pl.multiple_of((1 - core) * half + i * piece, piece), piece)]
        remote(at, at, o_send.at[i], o_recv.at[i], {"tp": partner}).wait_recv()
        o_copy(i).wait_send()


def one_call(
    ep, tp, share, part, packed, cap, routes, scale, gains, off, exp_rows, mix, wq, wk, wv,
    wg, wu, wd, wo,
):
    token_count, width = exp_rows.shape
    row_count, full = mix.shape
    heads = off.shape[0]
    head_size = wq.shape[0] // heads
    slots = ep * cap
    chips = tp // 2
    half = row_count // 2
    pieces = 4
    groups = 2 if ep % 2 == 0 else 1
    others = max(chips - 1, 1)
    channels = wo.shape[0]
    wide = chips == 2 and packed and ep % 2 == 0 and share % 2 == 0
    w_pieces = 8
    q_rows = part // 2 if packed else part
    q_stride = head_size if packed else 2 * head_size
    dma = pltpu.SemaphoreType.DMA
    vmem = pl.BlockSpec(memory_space=pltpu.VMEM)
    hbm = pl.BlockSpec(memory_space=pl.ANY)

    def held(*shape):
        return pltpu.VMEM(shape, jnp.bfloat16)

    def both(*shape):
        return [dma(shape), dma(shape)]

    return pl.pallas_call(
        functools.partial(kernel, (ep, tp, share, part, packed, cap)),
        out_shape=(
            pltpu.VMEM((row_count, full), jnp.bfloat16),
            pltpu.VMEM((token_count, width), jnp.bfloat16),
        ),
        in_specs=[vmem] * 5 + [hbm] * 8,
        out_specs=(vmem, vmem),
        scratch_shapes=[
            held(row_count, full), held(row_count, full), held(heads * q_stride, full),
            held(2 * heads * head_size, full), held(heads, row_count, 128),
            held(ep, q_rows, 128), held(ep, cap, width),
            pltpu.VMEM((ep, token_count), jnp.float32), pltpu.VMEM((ep, token_count), jnp.float32),
            held(slots, width),
            held(ep, row_count, 128), held(ep, q_rows, 128),
            held(slots + 16, full),
            held(*wg.shape), held(*wu.shape), held(*wd.shape),
            held(tp * channels if wide else channels, full),
            held(slots, full), held(chips, slots, width), held(others, slots, width),
            held(others, slots, width), held(slots, width),
            held(ep, q_rows, 128), held(ep, q_rows, 128), held(row_count, wo.shape[0]),
            held(*((16, 128) if wide else (half, full))),
            held(*((16, 128) if wide else (half, full))),
            held(*((1, 16, 128) if wide else (chips, half, full))),
            held(*((half, tp * channels) if wide else (16, 128))),
        ]
        + both(ep) + [dma((ep,))] + both(ep) + both(ep) + both(ep + 1) + both(chips, ep + 1)
        + both(chips, ep + 1) + both(chips, groups) + both(chips, ep) + both(ep) + both(ep)
        + both(1) + both(chips, pieces) + both(pieces) + both(tp) + both(w_pieces)
        + both(w_pieces) + both(4) + [dma((1 + 3 * heads,)), dma((4,))],
        compiler_params=pltpu.CompilerParams(
            collective_id=0, has_side_effects=True, vmem_limit_bytes=60 * 1024 * 1024
        ),
    )(routes, scale, gains, off, exp_rows, mix, wq, wk, wv, wg, wu, wd, wo)


def on_device(
    mix_rows,
    mix_gain,
    w_query,
    w_key,
    w_value,
    key_offset,
    w_out,
    out_gain,
    exp_rows,
    exp_gain,
    routes,
    route_weight,
    w_gate,
    w_up,
    w_down,
):
    ep = lax.axis_size("ep")
    tp = lax.axis_size("tp")
    row_count = mix_rows.shape[0]
    heads_here = key_offset.shape[0]
    head_size = w_query.shape[0] // heads_here
    share = ep // heads_here
    part = row_count // share
    packed = part % 32 == 0 and heads_here % 2 == 0
    token_count, top_count = routes.shape
    experts = w_gate.shape[0] * ep
    capacity = 4 * token_count * top_count // (3 * experts)
    gains = jnp.concatenate([mix_gain, out_gain, exp_gain]).astype(jnp.float32)
    gains = lax.optimization_barrier(gains)[None]
    if not packed:
        w_out = w_out.reshape(heads_here, head_size, -1)
        w_out = jnp.concatenate([jnp.zeros_like(w_out), w_out], axis=1)
        w_out = w_out.reshape(2 * heads_here * head_size, -1)
    mix_out, exp_out = one_call(
        ep, tp, share, part, packed, capacity, routes.T, route_weight.T, gains, key_offset,
        exp_rows, mix_rows, w_query, w_key, w_value, w_gate[0], w_up[0], w_down[0], w_out,
    )
    return (mix_out, exp_out)


def solution(mesh):
    placed = (
        P("ep", None),
        P(),
        P("tp", None),
        P("tp", None),
        P("tp", None),
        P("tp", None),
        P("tp", None),
        P(),
        P("ep", "tp"),
        P("tp"),
        P("ep", None),
        P("ep", None),
        P("ep", None, "tp"),
        P("ep", None, "tp"),
        P("ep", "tp", None),
    )
    return jax.shard_map(
        on_device,
        mesh=mesh,
        in_specs=placed,
        out_specs=(P("ep", None), P("ep", "tp")),
        check_vma=False,
    )
```

```python
import functools
import math

import jax
import jax.numpy as jnp
from jax import lax
from jax.experimental import pallas as pl
from jax.experimental.pallas import tpu as pltpu
from jax.sharding import PartitionSpec as P

EPSILON = 1e-06
CLAMP_LIMIT = 7.0
SILU_SHARPNESS = 1.702
MESH = pl.DeviceIdType.MESH


def normalize(numbers, gain):
    factor = lax.rsqrt(jnp.mean(numbers * numbers, axis=-1, keepdims=True) + EPSILON)
    return numbers * factor * gain.astype(jnp.float32)


def project(normed, weight):
    return lax.dot_general(
        normed, weight, (((1,), (1,)), ((), ())), preferred_element_type=jnp.float32
    )


def gated_units(gate_pre, up_pre):
    gate_part = jnp.minimum(gate_pre, CLAMP_LIMIT)
    up_part = jnp.clip(up_pre, -CLAMP_LIMIT, CLAMP_LIMIT)
    return (up_part + 1.0) * (gate_part * jax.nn.sigmoid(SILU_SHARPNESS * gate_part))


def stick_block(q, kv, off, carry, acc, later, visible):
    scores = (
        lax.dot_general(q, kv, (((1,), (1,)), ((), ())), preferred_element_type=jnp.float32) + off
    )
    keep = -(jnp.maximum(scores, 0.0) + jnp.log(1.0 + jnp.exp(-jnp.abs(scores))))
    own = scores + keep
    if visible is not None:
        keep = jnp.where(visible, keep, 0.0)
    beyond = jnp.dot(keep.astype(jnp.bfloat16), later, preferred_element_type=jnp.float32)
    weights = jnp.exp(own + beyond + carry)
    if visible is not None:
        weights = jnp.where(visible, weights, 0.0)
    acc = acc + jnp.dot(weights.astype(jnp.bfloat16), kv, preferred_element_type=jnp.float32)
    return carry + jnp.sum(keep, axis=1, keepdims=True), acc


def kernel(
    dims, routes_ref, scale_ref, gains_ref, off_ref, exp_ref, mix_hbm, wq_hbm, wk_hbm, wv_hbm,
    wg_hbm, wu_hbm, wd_hbm, wo_hbm,
    out_ref, exp_out_ref,
    mix_ref, normed_ref, wq_ref, wkv_ref, kv_ref, q_ref, x_out, key_ref, weight_ref, ret_ref,
    kv_all, q_all, seg_ref, wg_ref, wu_ref, wd_ref, wo_ref, sum_ref, e_got, e_pair, e_y, e_fin,
    att_ref, att_all, att_rows, m_send, m_got, m_sum, att_wide,
    kv_send, kv_recv, k_send, q_send, q_recv, x_send, x_recv, p_send, p_recv, g_send, g_recv,
    f_send, f_recv, d_send, d_recv, y_send, y_recv, z_send, z_recv, a_send, a_recv,
    h_send, h_recv, v_send, v_recv, o_send, o_recv, b_send, b_recv, wy_send, wy_recv,
    wx_send, wx_recv, wd_send, wd_recv, mix_sem, w_sem,
):
    ep, tp, share, part, packed, cap = dims
    chips = tp // 2
    heads = ep // share
    me = lax.axis_index("ep")
    mt = lax.axis_index("tp")
    core = lax.rem(mt, 2)
    partner = mt + 1 - 2 * core
    token_count, width = exp_ref.shape
    full = seg_ref.shape[1]
    head_size = wk_hbm.shape[0] // heads
    tail_rows = seg_ref.shape[0] - ep * cap
    block = kv_ref.shape[1]
    half = out_ref.shape[0] // 2
    pieces = o_send.shape[0]
    piece = half // pieces
    groups = d_send.shape[1]
    per = ep // groups
    channels = wo_hbm.shape[0]
    wide = wo_ref.shape[0] > channels
    mine_at = pl.multiple_of(mt * channels, 128) if wide else 0
    w_pieces = wy_send.shape[0]
    w_rows = channels // 2 // w_pieces

    def peer(s):
        return lax.rem(me + s, ep)

    def before(s):
        return lax.rem(me - s + ep, ep)

    def other(k):
        return lax.rem(mt + 2 * k, tp)

    stride = head_size if packed else 2 * head_size
    places = [(mix_hbm, mix_ref)]
    for h in range(heads):
        one = pl.ds(h * head_size, head_size)
        places.append((wk_hbm.at[one], wkv_ref.at[pl.ds(2 * h * head_size, head_size)]))
        places.append((wv_hbm.at[one], wkv_ref.at[pl.ds((2 * h + 1) * head_size, head_size)]))
        places.append((wq_hbm.at[one], wq_ref.at[pl.ds(h * stride, head_size)]))
    mix_loads = [
        pltpu.make_async_copy(src, dst, mix_sem.at[i]) for i, (src, dst) in enumerate(places)
    ]
    for copy in mix_loads:
        copy.start()
    wo_place = wo_ref.at[pl.ds(mine_at, channels)]
    weights = [
        pltpu.make_async_copy(src, dst, w_sem.at[i])
        for i, (src, dst) in enumerate(
            [(wo_hbm, wo_place), (wg_hbm, wg_ref), (wu_hbm, wu_ref), (wd_hbm, wd_ref)]
        )
    ]
    for copy in weights:
        copy.start()

    barrier = pltpu.get_barrier_semaphore()

    def greet(s, _):
        pl.semaphore_signal(barrier, inc=1, device_id={"ep": peer(s)}, device_id_type=MESH)
        return 0

    lax.fori_loop(1, ep, greet, 0)
    pl.semaphore_signal(barrier, inc=1, device_id={"tp": partner}, device_id_type=MESH)
    for k in range(1, chips):
        pl.semaphore_signal(barrier, inc=1, device_id={"tp": other(k)}, device_id_type=MESH)

    def remote(src, dst, send, recv, where):
        return pltpu.make_async_remote_copy(
            src_ref=src, dst_ref=dst, send_sem=send, recv_sem=recv,
            device_id=where, device_id_type=MESH,
        )

    def rows(s):
        return pl.ds(s * cap, cap)

    def columns(t):
        return pl.ds(pl.multiple_of(t * width, 128), width)

    def x_copy(s):
        return remote(
            x_out.at[s], seg_ref.at[rows(s), columns(mt)], x_send.at[s], x_recv.at[s],
            {"ep": peer(s)},
        )

    def kv_copy(dest, slot):
        return remote(
            kv_ref.at[dest // share], kv_all.at[slot], kv_send.at[dest], kv_recv.at[slot],
            {"ep": dest},
        )

    def k_copy(slot):
        return remote(
            kv_all.at[slot], kv_all.at[slot], k_send.at[slot], kv_recv.at[slot], {"ep": twin}
        )

    def q_copy(dest, slot):
        return remote(
            q_ref.at[dest], q_all.at[slot], q_send.at[dest], q_recv.at[slot], {"ep": dest}
        )

    def w_part(t, half_of, i):
        at = pl.multiple_of(t * channels + half_of * (channels // 2) + i * w_rows, 16)
        return wo_ref.at[pl.ds(at, w_rows)]

    def w_half(t, half_of):
        at = pl.multiple_of(t * channels + half_of * (channels // 2), 16)
        return wo_ref.at[pl.ds(at, channels // 2)]

    parity = lax.rem(me, 2)

    def wy_copy(i):
        at = w_part(mt, parity, i)
        return remote(at, at, wy_send.at[i], wy_recv.at[i], {"tp": other(1)})

    def wx_copy(i):
        at = w_part(other(1), parity, i)
        return remote(at, at, wx_send.at[i], wx_recv.at[i], {"ep": twin})

    def wd_copy(i):
        at = w_half(mt if i < 2 else other(1), i if i < 2 else (parity if i == 2 else 1 - parity))
        return remote(at, at, wd_send.at[i], wd_recv.at[i], {"tp": partner})

    def w_across(first, last):
        for i in range(first, last):
            wy_copy(i).wait_recv()
            wx_copy(i).start()
        if last == w_pieces:
            wd_copy(2).start()

    def w_along():
        for i in range(w_pieces):
            wx_copy(i).wait_recv()
        wd_copy(3).start()

    tail = pl.ds(ep * cap, tail_rows)
    step = 2 if share % 2 == 0 else 1
    twin = me + 1 - 2 * lax.rem(me, 2)

    def w_start(first, last):
        for i in range(first, last):
            wy_copy(i).start()

    w_first = 5 if ep == 8 else w_pieces
    weights[0].wait()
    pl.semaphore_wait(barrier, ep - 1 + 1 + chips - 1)
    if wide:
        w_start(0, w_first)
        for i in range(2):
            wd_copy(i).start()

    expert_ids = lax.broadcasted_iota(jnp.int32, (ep, token_count), 0)
    chosen = jnp.zeros((ep, token_count), jnp.float32)
    weight = jnp.zeros((ep, token_count), jnp.float32)
    for k in range(routes_ref.shape[0]):
        hit = routes_ref[k : k + 1, :] == expert_ids
        chosen = jnp.where(hit, 1.0, chosen)
        weight = jnp.where(hit, scale_ref[k : k + 1, :], weight)
    earlier = (
        lax.broadcasted_iota(jnp.int32, (token_count, token_count), 0)
        < lax.broadcasted_iota(jnp.int32, (token_count, token_count), 1)
    ).astype(jnp.float32)
    slot_of = jnp.dot(chosen, earlier, preferred_element_type=jnp.float32)
    key_ref[...] = jnp.where(chosen > 0.0, slot_of, -1.0)
    weight_ref[...] = weight
    slot_ids = lax.broadcasted_iota(jnp.int32, (cap, token_count), 0).astype(jnp.float32)

    def placed(e):
        return key_ref[pl.ds(e, 1), :] == slot_ids

    def routed(s):
        picked = jnp.where(placed(peer(s)), 1.0, 0.0).astype(jnp.bfloat16)
        return jnp.dot(picked, exp_ref[...], preferred_element_type=jnp.float32).astype(
            jnp.bfloat16
        )

    exp_gain = gains_ref[:, 2 * full :]
    seg_ref[tail, columns(mt)] = jnp.broadcast_to(exp_gain, (tail_rows, width)).astype(jnp.bfloat16)
    ahead = per if ep == 8 else ep

    def send_x(first, last):
        for s in range(first, last):
            x_out[s] = routed(s)
            x_copy(s).start()

    send_x(1, ahead)
    seg_ref[rows(0), columns(mt)] = routed(0)

    def rows_of(n):
        return tail if n == ep else rows(n)

    def p_copy(n):
        at = seg_ref.at[rows_of(n), columns(mt)]
        return remote(at, at, p_send.at[n], p_recv.at[n], {"tp": partner})

    def g_copy(n, k):
        at = seg_ref.at[rows_of(n), columns(mt)]
        return remote(at, at, g_send.at[k, n], g_recv.at[k, n], {"tp": other(k)})

    def f_copy(n, k):
        at = seg_ref.at[rows_of(n), columns(lax.rem(mt - 2 * k + tp, tp))]
        return remote(at, at, f_send.at[k, n], f_recv.at[k, n], {"tp": partner})

    def spread(n):
        if 0 < n < ep:
            x_copy(n).wait_recv()
        for k in range(1, chips):
            g_copy(n, k).start()
        p_copy(n).start()

    def forward(n):
        for k in range(1, chips):
            g_copy(n, k).wait_recv()
            f_copy(n, k).start()

    def gathered(n):
        p_copy(n).wait_recv()
        for k in range(1, chips):
            f_copy(n, k).wait_recv()

    def d_copy(k, g):
        at = pl.ds(g * per * cap, per * cap)
        return remote(
            sum_ref.at[at, columns(lax.rem(partner + 2 * k, tp))], e_got.at[k, at],
            d_send.at[k, g], d_recv.at[k, g], {"tp": partner},
        )

    def y_copy(k, s):
        return remote(
            e_pair.at[k - 1, rows(s)], e_y.at[k - 1, rows(s)], y_send.at[k, s],
            y_recv.at[k, s], {"tp": other(k)},
        )

    def z_copy(s):
        place = ret_ref.at[pl.ds(pl.multiple_of(me * cap, cap), cap)]
        return remote(
            e_fin.at[rows(s)], place, z_send.at[s], z_recv.at[s], {"ep": before(s)}
        )

    def z_arrived(s):
        place = ret_ref.at[pl.ds(pl.multiple_of(peer(s) * cap, cap), cap)]
        return remote(
            e_fin.at[rows(s)], place, z_send.at[s], z_recv.at[s], {"ep": before(s)}
        )

    def expert(g):
        at = pl.ds(g * per * cap, per * cap)
        gains = seg_ref[tail, :][:1]
        segment = normalize(seg_ref[at, :].astype(jnp.float32), gains).astype(jnp.bfloat16)
        gate_pre = jnp.dot(segment, wg_ref[...], preferred_element_type=jnp.float32)
        up_pre = jnp.dot(segment, wu_ref[...], preferred_element_type=jnp.float32)
        hidden = gated_units(gate_pre, up_pre).astype(jnp.bfloat16)
        sum_ref[at, :] = jnp.dot(
            hidden, wd_ref[...], preferred_element_type=jnp.float32
        ).astype(jnp.bfloat16)
        for k in list(range(1, chips)) + [0]:
            d_copy(k, g).start()

    def pair_start(g):
        for k in range(1, chips):
            d_copy(k, g).wait_recv()
        pair_rows(range(g * per, g * per + per // 2))

    def pair_end(g):
        pair_rows(range(g * per + per // 2, (g + 1) * per))
        d_copy(0, g).wait_recv()

    def pair(g):
        pair_start(g)
        pair_end(g)

    def pair_rows(these):
        for s in these:
            for k in range(1, chips):
                mine = sum_ref[rows(s), columns(other(k))].astype(jnp.float32)
                both = mine + e_got[k, rows(s), :].astype(jnp.float32)
                e_pair[k - 1, rows(s), :] = both.astype(jnp.bfloat16)
                y_copy(k, s).start()

    early = ep - 1

    def fin(s):
        total = sum_ref[rows(s), columns(mt)].astype(jnp.float32)
        total = total + e_got[0, rows(s), :].astype(jnp.float32)
        for k in range(1, chips):
            y_copy(k, s).wait_recv()
            total = total + e_y[k - 1, rows(s), :].astype(jnp.float32)
        if s > 0:
            e_fin[rows(s), :] = total.astype(jnp.bfloat16)
        else:
            ret_ref[pl.ds(pl.multiple_of(me * cap, cap), cap), :] = total.astype(jnp.bfloat16)
        if 0 < s <= early:
            z_copy(s).start()

    def make_mix():
        for copy in mix_loads:
            copy.wait()
        gain = gains_ref[:, :full]
        chunk = min(64, block)
        for r in range(0, block, chunk):
            at = pl.ds(r, chunk)
            normed_ref[at, :] = normalize(mix_ref[at, :].astype(jnp.float32), gain).astype(
                jnp.bfloat16
            )
        if not packed:
            for h in range(heads):
                at = pl.ds(h * stride + head_size, head_size)
                wq_ref[at, :] = jnp.zeros((head_size, full), jnp.bfloat16)
        both = project(normed_ref[...], wkv_ref[...])
        for h in range(heads):
            kv_ref[h] = both[:, h * 128 : (h + 1) * 128].astype(jnp.bfloat16)
        kv_all[me] = kv_ref[me // share]
        for i in range(step, ep, step):
            kv_copy(lax.rem(me + i, ep), me).start()
        if step == 2:
            k_copy(me).start()
        q = project(normed_ref[...], wq_ref[...]) * (1.0 / math.sqrt(head_size))
        for r in range(share):
            one = q[r * part : (r + 1) * part]
            if packed:
                first, second = one[: part // 2], one[part // 2 :]
                for h in range(0, heads, 2):
                    at = slice(h * head_size, (h + 2) * head_size)
                    left, right = first[:, at], second[:, at]
                    even = jnp.where(lane < 64, left, pltpu.roll(right, 64, 1))
                    odd = jnp.where(lane < 64, pltpu.roll(left, 64, 1), right)
                    q_ref[h * share + r] = even.astype(jnp.bfloat16)
                    q_ref[(h + 1) * share + r] = odd.astype(jnp.bfloat16)
            else:
                for h in range(heads):
                    q_ref[h * share + r] = one[:, h * 128 : (h + 1) * 128].astype(jnp.bfloat16)
        q_all[me] = q_ref[me]

    def pass_on(i):
        slot = lax.rem(me - i + ep, ep)
        kv_copy(peer(1), slot).wait_recv()
        k_copy(slot).start()

    lane = lax.broadcasted_iota(jnp.int32, (1, 128), 1)
    spread(ep)
    spread(0)
    make_mix()

    def send_q(s, _):
        q_copy(peer(s), me).start()
        return 0

    lax.fori_loop(1, ep, send_q, 0)

    def kv_forward():
        if step == 2:
            for i in range(2, ep, 2):
                pass_on(i)

    def collect(g):
        if g == 0:
            gathered(ep)
            for copy in weights[1:]:
                copy.wait()
        for s in range(g * per, (g + 1) * per):
            gathered(s)

    def q_wait(s, _):
        q_copy(peer(s), before(s)).wait_recv()
        return 0

    def run_expert(g):
        collect(g)
        expert(g)

    def first_forward():
        forward(ep)
        forward(0)

    def fins(g):
        for s in range(g * per, (g + 1) * per):
            fin(s)

    tasks = []

    def add(when, act, *args):
        tasks.append((when, functools.partial(act, *args)))

    if ep == 8:
        add(-1, spread, 1)
        add(-1, spread, 2)
        add(-1, spread, 3)
        if wide:
            add(-1, w_start, w_first, w_pieces)
        add(-1, kv_forward)
        add(-1, send_x, ahead, ep)
        if wide:
            add(-1, w_across, 0, w_first)
        add(-1, first_forward)
        add(-1, forward, 1)
        add(0, forward, 2)
        add(1, forward, 3)
        add(2, spread, 4)
        add(2, run_expert, 0)
        add(2, spread, 5)
        if wide:
            add(4, w_across, w_first, w_pieces)
        add(3, spread, 6)
        add(4, spread, 7)
        add(5, forward, 4)
        add(5, pair, 0)
        add(7, forward, 5)
        add(8, forward, 6)
        add(8, forward, 7)
        add(8, run_expert, 1)
        add(8, pair_start, 1)
        add(9, pair_end, 1)
        add(9, fins, 0)
        if wide:
            add(9, w_along)
    else:
        add(-1, kv_forward)
        for n in range(1, ep):
            add(ep, spread, n)
        add(ep, first_forward)
        for n in range(1, ep):
            add(ep, forward, n)
        for g in range(groups):
            add(ep, run_expert, g)
            if g > 0:
                add(ep, pair, g - 1)
        if wide:
            add(ep, w_across, 0, w_pieces)
            add(ep, w_along)
        for g in range(groups - 1):
            add(ep, fins, g)

    for when, act in tasks:
        if when < 0:
            act()
    lax.fori_loop(1, ep, q_wait, 0)

    def queries(i):
        both = q_all[i].astype(jnp.float32)
        if packed:
            both = jnp.concatenate([both, pltpu.roll(both, 64, 1)], axis=0)
        return jnp.where(lane < 64, both, 0.0).astype(jnp.bfloat16)

    later = (
        lax.broadcasted_iota(jnp.int32, (block, block), 0)
        > lax.broadcasted_iota(jnp.int32, (block, block), 1)
    ).astype(jnp.float32).astype(jnp.bfloat16)
    row = lax.broadcasted_iota(jnp.int32, (part, block), 0) + lax.rem(me, share) * part
    visible = lax.broadcasted_iota(jnp.int32, (part, block), 1) < row
    carry = acc = q_rest = None
    for n in range(ep):
        j = ep - 1 - n

        @pl.when((me != j) if step == 1 else (lax.rem(me, 2) != j % 2))
        def _():
            kv_copy(peer(1), j).wait_recv()

        kv = kv_all[j]
        off = off_ref[pl.ds(me // share, 1), j * block : (j + 1) * block]
        q = queries(j)
        zero_carry = jnp.zeros((part, 1), jnp.float32)
        zero_acc = jnp.zeros((part, 128), jnp.float32)
        new_carry, new_acc = stick_block(q, kv, off, zero_carry, zero_acc, later, visible)
        if n == 0:
            carry, acc, q_rest = new_carry, new_acc, q
        else:
            carry, acc = stick_block(q_rest, kv, off, carry, acc, later, None)
            carry = jnp.concatenate([new_carry, carry], axis=0)
            acc = jnp.concatenate([new_acc, acc], axis=0)
            q_rest = jnp.concatenate([q, q_rest], axis=0)
        for when, act in tasks:
            if when == n:
                act()
    for i in range(ep):
        block_out = acc[i * part : (i + 1) * part]
        if packed:
            middle = part // 2
            block_out = jnp.where(
                lane < 64, pltpu.roll(block_out[:middle], 64, 1), block_out[middle:]
            )
        att_ref[i] = block_out.astype(jnp.bfloat16)

    def a_copy(dest, slot):
        return remote(
            att_ref.at[dest], att_all.at[slot], a_send.at[dest], a_recv.at[slot], {"ep": dest}
        )

    def start_a(s, _):
        a_copy(peer(s), me).start()
        return 0

    lax.fori_loop(1, ep, start_a, 0)
    att_all[me] = att_ref[me]
    for when, act in tasks:
        if when == ep:
            act()

    def wait_a(s, _):
        a_copy(peer(s), before(s)).wait_recv()
        return 0

    lax.fori_loop(1, ep, wait_a, 0)
    late = groups - 1
    for r in range(share):
        got = [att_all[h * share + r].astype(jnp.float32) for h in range(heads)]
        if packed:
            upper = []
            lower = []
            for h in range(0, heads, 2):
                upper.append(jnp.where(lane < 64, got[h], pltpu.roll(got[h + 1], 64, 1)))
                lower.append(jnp.where(lane < 64, pltpu.roll(got[h], 64, 1), got[h + 1]))
            both = jnp.concatenate(
                [jnp.concatenate(upper, axis=1), jnp.concatenate(lower, axis=1)], axis=0
            )
        else:
            both = []
            for h in range(heads):
                both.append(jnp.where(lane < 64, 0.0, got[h]))
            both = jnp.concatenate(both, axis=1)
        att_rows[pl.ds(r * part, part), :] = both.astype(jnp.bfloat16)

    def half_rows(c):
        return pl.ds(pl.multiple_of(c * half, half), half)

    def o_copy(i):
        at = out_ref.at[pl.ds(pl.multiple_of(core * half + i * piece, piece), piece)]
        return remote(at, at, o_send.at[i], o_recv.at[i], {"tp": partner})

    gain = gains_ref[:, full : 2 * full]

    def combine():
        total = jnp.zeros((token_count, width), jnp.float32)
        for s in range(ep):
            if s > 0:
                z_arrived(s).wait_recv()
            e = peer(s)
            spread_to = jnp.where(placed(e), weight_ref[pl.ds(e, 1), :], 0.0)
            high = spread_to.astype(jnp.bfloat16).astype(jnp.float32)
            both = jnp.concatenate([high, spread_to - high], axis=0).T.astype(jnp.bfloat16)
            got = ret_ref[pl.ds(pl.multiple_of(e * cap, cap), cap), :]
            for low in range(2):
                total = total + jnp.dot(
                    both[:, low * cap : (low + 1) * cap], got, preferred_element_type=jnp.float32
                )
        exp_out_ref[...] = total.astype(jnp.bfloat16)

    def b_copy(j):
        dest = lax.rem(mt + j, tp)
        return remote(
            att_rows.at[half_rows(lax.rem(dest, 2))],
            att_wide.at[:, pl.ds(mine_at, channels)],
            b_send.at[j], b_recv.at[j], {"tp": dest},
        )

    def h_copy():
        return remote(m_send, m_got, h_send.at[0], h_recv.at[0], {"tp": partner})

    def v_copy(k, i):
        at = pl.ds(i * piece, piece)
        return remote(
            m_sum.at[0, at], m_sum.at[k, at], v_send.at[k, i], v_recv.at[k, i],
            {"tp": other(k)},
        )

    def publish(i, total):
        own_rows = pl.ds(pl.multiple_of(core * half + i * piece, piece), piece)
        out_ref[own_rows, :] = normalize(total, gain).astype(jnp.bfloat16)
        o_copy(i).start()

    if wide:
        for j in range(1, tp):
            b_copy(j).start()
        att_wide[:, pl.ds(mine_at, channels)] = att_rows[half_rows(core), :]
        for when, act in tasks:
            if when == ep + 1:
                act()
        for i in range(4):
            wd_copy(i).wait_recv()
        fins(late)
        for j in range(1, tp):
            b_copy(j).wait_recv()
        for i in range(pieces):
            total = jnp.dot(
                att_wide[i * piece : (i + 1) * piece, :], wo_ref[...],
                preferred_element_type=jnp.float32,
            )
            publish(i, total)
        for s in range(early + 1, ep):
            z_copy(s).start()
        combine()
    else:
        pair(late)
        fins(late)
        for s in range(early + 1, ep):
            z_copy(s).start()
        m_send[...] = jnp.dot(
            att_rows[half_rows(1 - core), :], wo_ref[...], preferred_element_type=jnp.float32
        ).astype(jnp.bfloat16)
        h_copy().start()
        mine = jnp.dot(
            att_rows[half_rows(core), :], wo_ref[...], preferred_element_type=jnp.float32
        )
        h_copy().wait_recv()
        for i in range(pieces):
            at = pl.ds(i * piece, piece)
            both = mine[i * piece : (i + 1) * piece] + m_got[at, :].astype(jnp.float32)
            m_sum[0, at, :] = both.astype(jnp.bfloat16)
            for k in range(1, chips):
                v_copy(k, i).start()
        combine()
        for i in range(pieces):
            at = pl.ds(i * piece, piece)
            for k in range(1, chips):
                v_copy(k, i).wait_recv()
            total = jnp.zeros((piece, out_ref.shape[1]), jnp.float32)
            for chip in range(chips):
                slot = lax.rem(mt // 2 - chip + chips, chips)
                total = total + m_sum[slot, at, :].astype(jnp.float32)
            publish(i, total)

    if wide:
        for j in range(1, tp):
            b_copy(j).wait_send()
        for i in range(w_pieces):
            wy_copy(i).wait_send()
            wx_copy(i).wait_send()
        for i in range(4):
            wd_copy(i).wait_send()
    else:
        h_copy().wait_send()
        for k in range(1, chips):
            for i in range(pieces):
                v_copy(k, i).wait_send()
    for n in range(ep + 1):
        p_copy(n).wait_send()
        for k in range(1, chips):
            g_copy(n, k).wait_send()
            f_copy(n, k).wait_send()
    for k in range(chips):
        for g in range(groups):
            d_copy(k, g).wait_send()
    for k in range(1, chips):
        for s in range(ep):
            y_copy(k, s).wait_send()
    for s in range(1, ep):
        x_copy(s).wait_send()
        z_copy(s).wait_send()

    def finish(s, _):
        q_copy(peer(s), me).wait_send()
        a_copy(peer(s), me).wait_send()
        return 0

    lax.fori_loop(1, ep, finish, 0)
    for i in range(step, ep, step):
        kv_copy(lax.rem(me + i, ep), me).wait_send()
    if step == 2:
        for i in range(0, ep, 2):
            k_copy(lax.rem(me - i + ep, ep)).wait_send()
    for i in range(pieces):
        at = out_ref.at[pl.ds(pl.multiple_of((1 - core) * half + i * piece, piece), piece)]
        remote(at, at, o_send.at[i], o_recv.at[i], {"tp": partner}).wait_recv()
        o_copy(i).wait_send()


def one_call(
    ep, tp, share, part, packed, cap, routes, scale, gains, off, exp_rows, mix, wq, wk, wv,
    wg, wu, wd, wo,
):
    token_count, width = exp_rows.shape
    row_count, full = mix.shape
    heads = off.shape[0]
    head_size = wq.shape[0] // heads
    slots = ep * cap
    chips = tp // 2
    half = row_count // 2
    pieces = 4
    groups = 2 if ep % 2 == 0 else 1
    others = max(chips - 1, 1)
    channels = wo.shape[0]
    wide = chips == 2 and packed and ep % 2 == 0 and share % 2 == 0
    w_pieces = 8
    q_rows = part // 2 if packed else part
    q_stride = head_size if packed else 2 * head_size
    dma = pltpu.SemaphoreType.DMA
    vmem = pl.BlockSpec(memory_space=pltpu.VMEM)
    hbm = pl.BlockSpec(memory_space=pl.ANY)

    def held(*shape):
        return pltpu.VMEM(shape, jnp.bfloat16)

    def both(*shape):
        return [dma(shape), dma(shape)]

    return pl.pallas_call(
        functools.partial(kernel, (ep, tp, share, part, packed, cap)),
        out_shape=(
            pltpu.VMEM((row_count, full), jnp.bfloat16),
            pltpu.VMEM((token_count, width), jnp.bfloat16),
        ),
        in_specs=[vmem] * 5 + [hbm] * 8,
        out_specs=(vmem, vmem),
        scratch_shapes=[
            held(row_count, full), held(row_count, full), held(heads * q_stride, full),
            held(2 * heads * head_size, full), held(heads, row_count, 128),
            held(ep, q_rows, 128), held(ep, cap, width),
            pltpu.VMEM((ep, token_count), jnp.float32), pltpu.VMEM((ep, token_count), jnp.float32),
            held(slots, width),
            held(ep, row_count, 128), held(ep, q_rows, 128),
            held(slots + 16, full),
            held(*wg.shape), held(*wu.shape), held(*wd.shape),
            held(tp * channels if wide else channels, full),
            held(slots, full), held(chips, slots, width), held(others, slots, width),
            held(others, slots, width), held(slots, width),
            held(ep, q_rows, 128), held(ep, q_rows, 128), held(row_count, wo.shape[0]),
            held(*((16, 128) if wide else (half, full))),
            held(*((16, 128) if wide else (half, full))),
            held(*((1, 16, 128) if wide else (chips, half, full))),
            held(*((half, tp * channels) if wide else (16, 128))),
        ]
        + both(ep) + [dma((ep,))] + both(ep) + both(ep) + both(ep + 1) + both(chips, ep + 1)
        + both(chips, ep + 1) + both(chips, groups) + both(chips, ep) + both(ep) + both(ep)
        + both(1) + both(chips, pieces) + both(pieces) + both(tp) + both(w_pieces)
        + both(w_pieces) + both(4) + [dma((1 + 3 * heads,)), dma((4,))],
        compiler_params=pltpu.CompilerParams(
            collective_id=0, has_side_effects=True, vmem_limit_bytes=60 * 1024 * 1024
        ),
    )(routes, scale, gains, off, exp_rows, mix, wq, wk, wv, wg, wu, wd, wo)


def on_device(
    mix_rows,
    mix_gain,
    w_query,
    w_key,
    w_value,
    key_offset,
    w_out,
    out_gain,
    exp_rows,
    exp_gain,
    routes,
    route_weight,
    w_gate,
    w_up,
    w_down,
):
    ep = lax.axis_size("ep")
    tp = lax.axis_size("tp")
    row_count = mix_rows.shape[0]
    heads_here = key_offset.shape[0]
    head_size = w_query.shape[0] // heads_here
    share = ep // heads_here
    part = row_count // share
    packed = part % 32 == 0 and heads_here % 2 == 0
    token_count, top_count = routes.shape
    experts = w_gate.shape[0] * ep
    capacity = 4 * token_count * top_count // (3 * experts)
    gains = jnp.concatenate([mix_gain, out_gain, exp_gain]).astype(jnp.float32)
    gains = lax.optimization_barrier(gains)[None]
    if not packed:
        w_out = w_out.reshape(heads_here, head_size, -1)
        w_out = jnp.concatenate([jnp.zeros_like(w_out), w_out], axis=1)
        w_out = w_out.reshape(2 * heads_here * head_size, -1)
    mix_out, exp_out = one_call(
        ep, tp, share, part, packed, capacity, routes.T, route_weight.T, gains, key_offset,
        exp_rows, mix_rows, w_query, w_key, w_value, w_gate[0], w_up[0], w_down[0], w_out,
    )
    return (mix_out, exp_out)


def solution(mesh):
    placed = (
        P("ep", None),
        P(),
        P("tp", None),
        P("tp", None),
        P("tp", None),
        P("tp", None),
        P("tp", None),
        P(),
        P("ep", "tp"),
        P("tp"),
        P("ep", None),
        P("ep", None),
        P("ep", None, "tp"),
        P("ep", None, "tp"),
        P("ep", "tp", None),
    )
    return jax.shard_map(
        on_device,
        mesh=mesh,
        in_specs=placed,
        out_specs=(P("ep", None), P("ep", "tp")),
        check_vma=False,
    )
```

```python
import functools
import math

import jax
import jax.numpy as jnp
from jax import lax
from jax.experimental import pallas as pl
from jax.experimental.pallas import tpu as pltpu
from jax.sharding import PartitionSpec as P

EPSILON = 1e-06
CLAMP_LIMIT = 7.0
SILU_SHARPNESS = 1.702
MESH = pl.DeviceIdType.MESH


def normalize(numbers, gain):
    factor = lax.rsqrt(jnp.mean(numbers * numbers, axis=-1, keepdims=True) + EPSILON)
    return numbers * factor * gain.astype(jnp.float32)


def project(normed, weight):
    return lax.dot_general(
        normed, weight, (((1,), (1,)), ((), ())), preferred_element_type=jnp.float32
    )


def gated_units(gate_pre, up_pre):
    gate_part = jnp.minimum(gate_pre, CLAMP_LIMIT)
    up_part = jnp.clip(up_pre, -CLAMP_LIMIT, CLAMP_LIMIT)
    return (up_part + 1.0) * (gate_part * jax.nn.sigmoid(SILU_SHARPNESS * gate_part))


def stick_block(q, kv, off, carry, acc, later, visible):
    scores = (
        lax.dot_general(q, kv, (((1,), (1,)), ((), ())), preferred_element_type=jnp.float32) + off
    )
    keep = -(jnp.maximum(scores, 0.0) + jnp.log(1.0 + jnp.exp(-jnp.abs(scores))))
    own = scores + keep
    if visible is not None:
        keep = jnp.where(visible, keep, 0.0)
    beyond = jnp.dot(keep.astype(jnp.bfloat16), later, preferred_element_type=jnp.float32)
    weights = jnp.exp(own + beyond + carry)
    if visible is not None:
        weights = jnp.where(visible, weights, 0.0)
    acc = acc + jnp.dot(weights.astype(jnp.bfloat16), kv, preferred_element_type=jnp.float32)
    return carry + jnp.sum(keep, axis=1, keepdims=True), acc


def kernel(
    dims, routes_ref, scale_ref, gains_ref, off_ref, exp_ref, mix_hbm, wq_hbm, wk_hbm, wv_hbm,
    wg_hbm, wu_hbm, wd_hbm, wo_hbm,
    out_ref, exp_out_ref,
    mix_ref, normed_ref, wq_ref, wkv_ref, kv_ref, q_ref, x_out, key_ref, weight_ref, ret_ref,
    kv_all, q_all, seg_ref, wg_ref, wu_ref, wd_ref, wo_ref, sum_ref, e_got, e_pair, e_y, e_fin,
    att_ref, att_all, att_rows, m_send, m_got, m_sum, att_wide, mix_back,
    kv_send, kv_recv, k_send, q_send, q_recv, x_send, x_recv, p_send, p_recv, g_send, g_recv,
    f_send, f_recv, d_send, d_recv, y_send, y_recv, z_send, z_recv, a_send, a_recv,
    h_send, h_recv, v_send, v_recv, o_send, o_recv, b_send, b_recv, wy_send, wy_recv,
    wx_send, wx_recv, wd_send, wd_recv, mix_sem, w_sem,
):
    ep, tp, share, part, packed, cap = dims
    chips = tp // 2
    heads = ep // share
    me = lax.axis_index("ep")
    mt = lax.axis_index("tp")
    core = lax.rem(mt, 2)
    partner = mt + 1 - 2 * core
    token_count, width = exp_ref.shape
    full = seg_ref.shape[1]
    head_size = wk_hbm.shape[0] // heads
    tail_rows = seg_ref.shape[0] - ep * cap
    block = kv_ref.shape[1]
    half = out_ref.shape[0] // 2
    pieces = o_send.shape[0]
    piece = half // pieces
    groups = d_send.shape[1]
    per = ep // groups
    spans = [(g * per, (g + 1) * per) for g in range(groups)]
    if ep == 8:
        spans = [(0, 4), (4, 6), (6, 8)]
    channels = wo_hbm.shape[0]
    wide = wo_ref.shape[0] > channels
    mine_at = pl.multiple_of(mt * channels, 128) if wide else 0
    w_pieces = wy_send.shape[0]
    w_rows = channels // 2 // w_pieces

    def peer(s):
        return lax.rem(me + s, ep)

    def before(s):
        return lax.rem(me - s + ep, ep)

    def other(k):
        return lax.rem(mt + 2 * k, tp)

    stride = head_size if packed else 2 * head_size
    places = [(mix_hbm, mix_ref)]
    for h in range(heads):
        one = pl.ds(h * head_size, head_size)
        places.append((wk_hbm.at[one], wkv_ref.at[pl.ds(2 * h * head_size, head_size)]))
        places.append((wv_hbm.at[one], wkv_ref.at[pl.ds((2 * h + 1) * head_size, head_size)]))
        places.append((wq_hbm.at[one], wq_ref.at[pl.ds(h * stride, head_size)]))
    mix_loads = [
        pltpu.make_async_copy(src, dst, mix_sem.at[i]) for i, (src, dst) in enumerate(places)
    ]
    for copy in mix_loads:
        copy.start()
    wo_place = wo_ref.at[pl.ds(mine_at, channels)]
    weights = [
        pltpu.make_async_copy(src, dst, w_sem.at[i])
        for i, (src, dst) in enumerate(
            [(wo_hbm, wo_place), (wg_hbm, wg_ref), (wu_hbm, wu_ref), (wd_hbm, wd_ref)]
        )
    ]
    for copy in weights:
        copy.start()

    barrier = pltpu.get_barrier_semaphore()

    def greet(s, _):
        pl.semaphore_signal(barrier, inc=1, device_id={"ep": peer(s)}, device_id_type=MESH)
        return 0

    lax.fori_loop(1, ep, greet, 0)
    pl.semaphore_signal(barrier, inc=1, device_id={"tp": partner}, device_id_type=MESH)
    for k in range(1, chips):
        pl.semaphore_signal(barrier, inc=1, device_id={"tp": other(k)}, device_id_type=MESH)

    def remote(src, dst, send, recv, where):
        return pltpu.make_async_remote_copy(
            src_ref=src, dst_ref=dst, send_sem=send, recv_sem=recv,
            device_id=where, device_id_type=MESH,
        )

    def rows(s):
        return pl.ds(s * cap, cap)

    def columns(t):
        return pl.ds(pl.multiple_of(t * width, 128), width)

    def x_copy(s):
        return remote(
            x_out.at[s], seg_ref.at[rows(s), columns(mt)], x_send.at[s], x_recv.at[s],
            {"ep": peer(s)},
        )

    def kv_copy(dest, slot):
        return remote(
            kv_ref.at[dest // share], kv_all.at[slot], kv_send.at[dest], kv_recv.at[slot],
            {"ep": dest},
        )

    def k_copy(slot):
        return remote(
            kv_all.at[slot], kv_all.at[slot], k_send.at[slot], kv_recv.at[slot], {"ep": twin}
        )

    def q_copy(dest, slot):
        return remote(
            q_ref.at[dest], q_all.at[slot], q_send.at[dest], q_recv.at[slot], {"ep": dest}
        )

    def w_part(t, half_of, i):
        at = pl.multiple_of(t * channels + half_of * (channels // 2) + i * w_rows, 16)
        return wo_ref.at[pl.ds(at, w_rows)]

    def w_half(t, half_of):
        at = pl.multiple_of(t * channels + half_of * (channels // 2), 16)
        return wo_ref.at[pl.ds(at, channels // 2)]

    parity = lax.rem(me, 2)

    def wy_copy(i):
        at = w_part(mt, parity, i)
        return remote(at, at, wy_send.at[i], wy_recv.at[i], {"tp": other(1)})

    def wx_copy(i):
        at = w_part(other(1), parity, i)
        return remote(at, at, wx_send.at[i], wx_recv.at[i], {"ep": twin})

    def wd_copy(i):
        at = w_half(mt if i < 2 else other(1), i if i < 2 else (parity if i == 2 else 1 - parity))
        return remote(at, at, wd_send.at[i], wd_recv.at[i], {"tp": partner})

    def w_across(first, last):
        for i in range(first, last):
            wy_copy(i).wait_recv()
            wx_copy(i).start()
        if last == w_pieces:
            wd_copy(2).start()

    def w_along():
        for i in range(w_pieces):
            wx_copy(i).wait_recv()
        wd_copy(3).start()

    tail = pl.ds(ep * cap, tail_rows)
    step = 2 if share % 2 == 0 else 1
    twin = me + 1 - 2 * lax.rem(me, 2)

    def w_start(first, last):
        for i in range(first, last):
            wy_copy(i).start()

    w_first = 5 if ep == 8 else w_pieces
    weights[0].wait()
    pl.semaphore_wait(barrier, ep - 1 + 1 + chips - 1)
    if wide:
        w_start(0, w_first)
        for i in range(2):
            wd_copy(i).start()

    expert_ids = lax.broadcasted_iota(jnp.int32, (ep, token_count), 0)
    chosen = jnp.zeros((ep, token_count), jnp.float32)
    weight = jnp.zeros((ep, token_count), jnp.float32)
    for k in range(routes_ref.shape[0]):
        hit = routes_ref[k : k + 1, :] == expert_ids
        chosen = jnp.where(hit, 1.0, chosen)
        weight = jnp.where(hit, scale_ref[k : k + 1, :], weight)
    earlier = (
        lax.broadcasted_iota(jnp.int32, (token_count, token_count), 0)
        < lax.broadcasted_iota(jnp.int32, (token_count, token_count), 1)
    ).astype(jnp.float32)
    slot_of = jnp.dot(chosen, earlier, preferred_element_type=jnp.float32)
    key_ref[...] = jnp.where(chosen > 0.0, slot_of, -1.0)
    weight_ref[...] = weight
    slot_ids = lax.broadcasted_iota(jnp.int32, (cap, token_count), 0).astype(jnp.float32)

    def placed(e):
        return key_ref[pl.ds(e, 1), :] == slot_ids

    def routed(s):
        picked = jnp.where(placed(peer(s)), 1.0, 0.0).astype(jnp.bfloat16)
        return jnp.dot(picked, exp_ref[...], preferred_element_type=jnp.float32).astype(
            jnp.bfloat16
        )

    exp_gain = gains_ref[2 * full :][None]
    seg_ref[tail, columns(mt)] = jnp.broadcast_to(exp_gain, (tail_rows, width)).astype(jnp.bfloat16)
    ahead = 4 if ep == 8 else ep

    def send_x(first, last):
        for s in range(first, last):
            x_out[s] = routed(s)
            x_copy(s).start()

    send_x(1, ahead)
    seg_ref[rows(0), columns(mt)] = routed(0)

    def rows_of(n):
        return tail if n == ep else rows(n)

    def p_copy(n):
        at = seg_ref.at[rows_of(n), columns(mt)]
        return remote(at, at, p_send.at[n], p_recv.at[n], {"tp": partner})

    def g_copy(n, k):
        at = seg_ref.at[rows_of(n), columns(mt)]
        return remote(at, at, g_send.at[k, n], g_recv.at[k, n], {"tp": other(k)})

    def f_copy(n, k):
        at = seg_ref.at[rows_of(n), columns(lax.rem(mt - 2 * k + tp, tp))]
        return remote(at, at, f_send.at[k, n], f_recv.at[k, n], {"tp": partner})

    def spread(n):
        if 0 < n < ep:
            x_copy(n).wait_recv()
        for k in range(1, chips):
            g_copy(n, k).start()
        p_copy(n).start()

    def forward(n):
        for k in range(1, chips):
            g_copy(n, k).wait_recv()
            f_copy(n, k).start()

    def gathered(n):
        p_copy(n).wait_recv()
        for k in range(1, chips):
            f_copy(n, k).wait_recv()

    def group_rows(g):
        return pl.ds(spans[g][0] * cap, (spans[g][1] - spans[g][0]) * cap)

    def d_copy(k, g):
        at = group_rows(g)
        return remote(
            sum_ref.at[at, columns(lax.rem(partner + 2 * k, tp))], e_got.at[k, at],
            d_send.at[k, g], d_recv.at[k, g], {"tp": partner},
        )

    def y_copy(k, s):
        return remote(
            e_pair.at[k - 1, rows(s)], e_y.at[k - 1, rows(s)], y_send.at[k, s],
            y_recv.at[k, s], {"tp": other(k)},
        )

    def z_copy(s):
        place = ret_ref.at[pl.ds(pl.multiple_of(me * cap, cap), cap)]
        return remote(
            e_fin.at[rows(s)], place, z_send.at[s], z_recv.at[s], {"ep": before(s)}
        )

    def z_arrived(s):
        place = ret_ref.at[pl.ds(pl.multiple_of(peer(s) * cap, cap), cap)]
        return remote(
            e_fin.at[rows(s)], place, z_send.at[s], z_recv.at[s], {"ep": before(s)}
        )

    def expert(g):
        at = group_rows(g)
        gains = seg_ref[tail, :][:1]
        segment = normalize(seg_ref[at, :].astype(jnp.float32), gains).astype(jnp.bfloat16)
        gate_pre = jnp.dot(segment, wg_ref[...], preferred_element_type=jnp.float32)
        up_pre = jnp.dot(segment, wu_ref[...], preferred_element_type=jnp.float32)
        hidden = gated_units(gate_pre, up_pre).astype(jnp.bfloat16)
        sum_ref[at, :] = jnp.dot(
            hidden, wd_ref[...], preferred_element_type=jnp.float32
        ).astype(jnp.bfloat16)
        for k in list(range(1, chips)) + [0]:
            d_copy(k, g).start()

    def pair_start(g):
        for k in range(1, chips):
            d_copy(k, g).wait_recv()
        pair_rows(range(*spans[g]))

    def pair_end(g):
        d_copy(0, g).wait_recv()

    def pair(g):
        pair_start(g)
        pair_end(g)

    def pair_rows(these):
        for s in these:
            for k in range(1, chips):
                mine = sum_ref[rows(s), columns(other(k))].astype(jnp.float32)
                both = mine + e_got[k, rows(s), :].astype(jnp.float32)
                e_pair[k - 1, rows(s), :] = both.astype(jnp.bfloat16)
                y_copy(k, s).start()

    early = ep - 1

    def fin(s):
        total = sum_ref[rows(s), columns(mt)].astype(jnp.float32)
        total = total + e_got[0, rows(s), :].astype(jnp.float32)
        for k in range(1, chips):
            y_copy(k, s).wait_recv()
            total = total + e_y[k - 1, rows(s), :].astype(jnp.float32)
        if s > 0:
            e_fin[rows(s), :] = total.astype(jnp.bfloat16)
        else:
            ret_ref[pl.ds(pl.multiple_of(me * cap, cap), cap), :] = total.astype(jnp.bfloat16)
        if 0 < s <= early:
            z_copy(s).start()

    def make_mix():
        for copy in mix_loads:
            copy.wait()
        gain = gains_ref[:full][None]
        chunk = min(64, block)
        for r in range(0, block, chunk):
            at = pl.ds(r, chunk)
            normed_ref[at, :] = normalize(mix_ref[at, :].astype(jnp.float32), gain).astype(
                jnp.bfloat16
            )
        if not packed:
            for h in range(heads):
                at = pl.ds(h * stride + head_size, head_size)
                wq_ref[at, :] = jnp.zeros((head_size, full), jnp.bfloat16)
        both = project(normed_ref[...], wkv_ref[...])
        for h in range(heads):
            kv_ref[h] = both[:, h * 128 : (h + 1) * 128].astype(jnp.bfloat16)
        kv_all[me] = kv_ref[me // share]
        for i in range(step, ep, step):
            kv_copy(lax.rem(me + i, ep), me).start()
        if step == 2:
            k_copy(me).start()
        q = project(normed_ref[...], wq_ref[...]) * (1.0 / math.sqrt(head_size))
        for r in range(share):
            one = q[r * part : (r + 1) * part]
            if packed:
                first, second = one[: part // 2], one[part // 2 :]
                for h in range(0, heads, 2):
                    at = slice(h * head_size, (h + 2) * head_size)
                    left, right = first[:, at], second[:, at]
                    even = jnp.where(lane < 64, left, pltpu.roll(right, 64, 1))
                    odd = jnp.where(lane < 64, pltpu.roll(left, 64, 1), right)
                    q_ref[h * share + r] = even.astype(jnp.bfloat16)
                    q_ref[(h + 1) * share + r] = odd.astype(jnp.bfloat16)
            else:
                for h in range(heads):
                    q_ref[h * share + r] = one[:, h * 128 : (h + 1) * 128].astype(jnp.bfloat16)
        q_all[me] = q_ref[me]

    def pass_on(i):
        slot = lax.rem(me - i + ep, ep)
        kv_copy(peer(1), slot).wait_recv()
        k_copy(slot).start()

    lane = lax.broadcasted_iota(jnp.int32, (1, 128), 1)
    spread(ep)
    spread(0)
    make_mix()

    def send_q(s, _):
        q_copy(peer(s), me).start()
        return 0

    lax.fori_loop(1, ep, send_q, 0)

    def kv_forward():
        if step == 2:
            for i in range(2, ep, 2):
                pass_on(i)

    def collect(g):
        if g == 0:
            gathered(ep)
            for copy in weights[1:]:
                copy.wait()
        for s in range(*spans[g]):
            gathered(s)

    def q_wait(s, _):
        q_copy(peer(s), before(s)).wait_recv()
        return 0

    def run_expert(g):
        collect(g)
        expert(g)

    def first_forward():
        forward(ep)
        forward(0)

    def fins(g):
        for s in range(*spans[g]):
            fin(s)

    def weigh():
        for s in range(ep):
            e = peer(s)
            spread_to = jnp.where(placed(e), weight_ref[pl.ds(e, 1), :], 0.0)
            high = spread_to.astype(jnp.bfloat16).astype(jnp.float32)
            both = jnp.concatenate([high, spread_to - high], axis=0)
            mix_back[s] = both.T.astype(jnp.bfloat16)

    tasks = []

    def add(when, act, *args):
        tasks.append((when, functools.partial(act, *args)))

    if ep == 8:
        add(-1, spread, 1)
        add(-1, spread, 2)
        add(-1, spread, 3)
        if wide:
            add(-1, w_start, w_first, w_pieces)
        add(-1, kv_forward)
        add(-1, send_x, ahead, ep)
        if wide:
            add(-1, w_across, 0, w_first)
        add(-1, first_forward)
        add(-1, forward, 1)
        add(0, forward, 2)
        add(1, forward, 3)
        add(2, spread, 4)
        add(2, run_expert, 0)
        add(2, spread, 5)
        if wide:
            add(4, w_across, w_first, w_pieces)
        add(3, spread, 6)
        add(4, spread, 7)
        add(4, forward, 4)
        add(5, pair, 0)
        add(5, forward, 5)
        add(7, forward, 6)
        add(8, run_expert, 1)
        add(8, forward, 7)
        add(8, weigh)
        add(8, pair_start, 1)
        add(8, run_expert, 2)
        add(8, fins, 0)
        add(8, pair_start, 2)
        add(9, pair_end, 1)
        add(9, pair_end, 2)
        add(9, fins, 1)
        if wide:
            add(9, w_along)
    else:
        add(-1, kv_forward)
        for n in range(1, ep):
            add(ep, spread, n)
        add(ep, first_forward)
        for n in range(1, ep):
            add(ep, forward, n)
        for g in range(groups):
            add(ep, run_expert, g)
            if g > 0:
                add(ep, pair, g - 1)
        if wide:
            add(ep, w_across, 0, w_pieces)
            add(ep, w_along)
        for g in range(groups - 1):
            add(ep, fins, g)
        add(ep, weigh)

    for when, act in tasks:
        if when < 0:
            act()
    lax.fori_loop(1, ep, q_wait, 0)

    def queries(i):
        both = q_all[i].astype(jnp.float32)
        if packed:
            both = jnp.concatenate([both, pltpu.roll(both, 64, 1)], axis=0)
        return jnp.where(lane < 64, both, 0.0).astype(jnp.bfloat16)

    later = (
        lax.broadcasted_iota(jnp.int32, (block, block), 0)
        > lax.broadcasted_iota(jnp.int32, (block, block), 1)
    ).astype(jnp.float32).astype(jnp.bfloat16)
    row = lax.broadcasted_iota(jnp.int32, (part, block), 0) + lax.rem(me, share) * part
    visible = lax.broadcasted_iota(jnp.int32, (part, block), 1) < row
    carry = acc = q_rest = None
    for n in range(ep):
        j = ep - 1 - n

        @pl.when((me != j) if step == 1 else (lax.rem(me, 2) != j % 2))
        def _():
            kv_copy(peer(1), j).wait_recv()

        kv = kv_all[j]
        off = off_ref[pl.ds(me // share, 1), j * block : (j + 1) * block]
        q = queries(j)
        zero_carry = jnp.zeros((part, 1), jnp.float32)
        zero_acc = jnp.zeros((part, 128), jnp.float32)
        new_carry, new_acc = stick_block(q, kv, off, zero_carry, zero_acc, later, visible)
        if n == 0:
            carry, acc, q_rest = new_carry, new_acc, q
        else:
            carry, acc = stick_block(q_rest, kv, off, carry, acc, later, None)
            carry = jnp.concatenate([new_carry, carry], axis=0)
            acc = jnp.concatenate([new_acc, acc], axis=0)
            q_rest = jnp.concatenate([q, q_rest], axis=0)
        for when, act in tasks:
            if when == n:
                act()
    for i in range(ep):
        block_out = acc[i * part : (i + 1) * part]
        if packed:
            middle = part // 2
            block_out = jnp.where(
                lane < 64, pltpu.roll(block_out[:middle], 64, 1), block_out[middle:]
            )
        att_ref[i] = block_out.astype(jnp.bfloat16)

    def a_copy(dest, slot):
        return remote(
            att_ref.at[dest], att_all.at[slot], a_send.at[dest], a_recv.at[slot], {"ep": dest}
        )

    def start_a(s, _):
        a_copy(peer(s), me).start()
        return 0

    lax.fori_loop(1, ep, start_a, 0)
    att_all[me] = att_ref[me]
    for when, act in tasks:
        if when == ep:
            act()

    def wait_a(s, _):
        a_copy(peer(s), before(s)).wait_recv()
        return 0

    lax.fori_loop(1, ep, wait_a, 0)
    late = groups - 1
    for r in range(share):
        got = [att_all[h * share + r].astype(jnp.float32) for h in range(heads)]
        if packed:
            upper = []
            lower = []
            for h in range(0, heads, 2):
                upper.append(jnp.where(lane < 64, got[h], pltpu.roll(got[h + 1], 64, 1)))
                lower.append(jnp.where(lane < 64, pltpu.roll(got[h], 64, 1), got[h + 1]))
            both = jnp.concatenate(
                [jnp.concatenate(upper, axis=1), jnp.concatenate(lower, axis=1)], axis=0
            )
        else:
            both = []
            for h in range(heads):
                both.append(jnp.where(lane < 64, 0.0, got[h]))
            both = jnp.concatenate(both, axis=1)
        att_rows[pl.ds(r * part, part), :] = both.astype(jnp.bfloat16)

    def half_rows(c):
        return pl.ds(pl.multiple_of(c * half, half), half)

    def o_copy(i):
        at = out_ref.at[pl.ds(pl.multiple_of(core * half + i * piece, piece), piece)]
        return remote(at, at, o_send.at[i], o_recv.at[i], {"tp": partner})

    gain = gains_ref[full : 2 * full][None]

    def combine():
        total = jnp.zeros((token_count, width), jnp.float32)
        for s in range(ep):
            if s > 0:
                z_arrived(s).wait_recv()
            got = ret_ref[pl.ds(pl.multiple_of(peer(s) * cap, cap), cap), :]
            total = total + jnp.dot(
                mix_back[s], jnp.concatenate([got, got], axis=0),
                preferred_element_type=jnp.float32,
            )
        exp_out_ref[...] = total.astype(jnp.bfloat16)

    def b_copy(j):
        dest = lax.rem(mt + j, tp)
        return remote(
            att_rows.at[half_rows(lax.rem(dest, 2))],
            att_wide.at[:, pl.ds(mine_at, channels)],
            b_send.at[j], b_recv.at[j], {"tp": dest},
        )

    def h_copy():
        return remote(m_send, m_got, h_send.at[0], h_recv.at[0], {"tp": partner})

    def v_copy(k, i):
        at = pl.ds(i * piece, piece)
        return remote(
            m_sum.at[0, at], m_sum.at[k, at], v_send.at[k, i], v_recv.at[k, i],
            {"tp": other(k)},
        )

    def publish(i, total):
        own_rows = pl.ds(pl.multiple_of(core * half + i * piece, piece), piece)
        out_ref[own_rows, :] = normalize(total, gain).astype(jnp.bfloat16)
        o_copy(i).start()

    def drain():
        if wide:
            for j in range(1, tp):
                b_copy(j).wait_send()
            for i in range(w_pieces):
                wy_copy(i).wait_send()
                wx_copy(i).wait_send()
            for i in range(4):
                wd_copy(i).wait_send()
        else:
            h_copy().wait_send()
            for k in range(1, chips):
                for i in range(pieces):
                    v_copy(k, i).wait_send()
        for n in range(ep + 1):
            p_copy(n).wait_send()
            for k in range(1, chips):
                g_copy(n, k).wait_send()
                f_copy(n, k).wait_send()
        for k in range(chips):
            for g in range(groups):
                d_copy(k, g).wait_send()
        for k in range(1, chips):
            for s in range(ep):
                y_copy(k, s).wait_send()
        for s in range(1, ep):
            x_copy(s).wait_send()

        def finish(s, _):
            q_copy(peer(s), me).wait_send()
            a_copy(peer(s), me).wait_send()
            return 0

        lax.fori_loop(1, ep, finish, 0)
        for i in range(step, ep, step):
            kv_copy(lax.rem(me + i, ep), me).wait_send()
        if step == 2:
            for i in range(0, ep, 2):
                k_copy(lax.rem(me - i + ep, ep)).wait_send()

    if wide:
        for j in range(1, tp):
            b_copy(j).start()
        att_wide[:, pl.ds(mine_at, channels)] = att_rows[half_rows(core), :]
        for when, act in tasks:
            if when == ep + 1:
                act()
        for i in range(4):
            wd_copy(i).wait_recv()
        fins(late)
        for j in range(1, tp):
            b_copy(j).wait_recv()
        for i in range(pieces):
            total = jnp.dot(
                att_wide[i * piece : (i + 1) * piece, :], wo_ref[...],
                preferred_element_type=jnp.float32,
            )
            publish(i, total)
        drain()
        combine()
    else:
        pair(late)
        fins(late)
        for s in range(early + 1, ep):
            z_copy(s).start()
        m_send[...] = jnp.dot(
            att_rows[half_rows(1 - core), :], wo_ref[...], preferred_element_type=jnp.float32
        ).astype(jnp.bfloat16)
        h_copy().start()
        mine = jnp.dot(
            att_rows[half_rows(core), :], wo_ref[...], preferred_element_type=jnp.float32
        )
        h_copy().wait_recv()
        for i in range(pieces):
            at = pl.ds(i * piece, piece)
            both = mine[i * piece : (i + 1) * piece] + m_got[at, :].astype(jnp.float32)
            m_sum[0, at, :] = both.astype(jnp.bfloat16)
            for k in range(1, chips):
                v_copy(k, i).start()
        combine()
        for i in range(pieces):
            at = pl.ds(i * piece, piece)
            for k in range(1, chips):
                v_copy(k, i).wait_recv()
            total = jnp.zeros((piece, out_ref.shape[1]), jnp.float32)
            for chip in range(chips):
                slot = lax.rem(mt // 2 - chip + chips, chips)
                total = total + m_sum[slot, at, :].astype(jnp.float32)
            publish(i, total)
        drain()

    for s in range(1, ep):
        z_copy(s).wait_send()
    for i in range(pieces):
        at = out_ref.at[pl.ds(pl.multiple_of((1 - core) * half + i * piece, piece), piece)]
        remote(at, at, o_send.at[i], o_recv.at[i], {"tp": partner}).wait_recv()
        o_copy(i).wait_send()


def one_call(
    ep, tp, share, part, packed, cap, routes, scale, gains, off, exp_rows, mix, wq, wk, wv,
    wg, wu, wd, wo,
):
    token_count, width = exp_rows.shape
    row_count, full = mix.shape
    heads = off.shape[0]
    head_size = wq.shape[0] // heads
    slots = ep * cap
    chips = tp // 2
    half = row_count // 2
    pieces = 4
    groups = 3 if ep == 8 else 2 if ep % 2 == 0 else 1
    others = max(chips - 1, 1)
    channels = wo.shape[0]
    wide = chips == 2 and packed and ep % 2 == 0 and share % 2 == 0
    pieces = 2 if wide else 4
    w_pieces = 8
    q_rows = part // 2 if packed else part
    q_stride = head_size if packed else 2 * head_size
    dma = pltpu.SemaphoreType.DMA
    vmem = pl.BlockSpec(memory_space=pltpu.VMEM)
    hbm = pl.BlockSpec(memory_space=pl.ANY)

    def held(*shape):
        return pltpu.VMEM(shape, jnp.bfloat16)

    def both(*shape):
        return [dma(shape), dma(shape)]

    return pl.pallas_call(
        functools.partial(kernel, (ep, tp, share, part, packed, cap)),
        out_shape=(
            pltpu.VMEM((row_count, full), jnp.bfloat16),
            pltpu.VMEM((token_count, width), jnp.bfloat16),
        ),
        in_specs=[vmem] * 5 + [hbm] * 8,
        out_specs=(vmem, vmem),
        scratch_shapes=[
            held(row_count, full), held(row_count, full), held(heads * q_stride, full),
            held(2 * heads * head_size, full), held(heads, row_count, 128),
            held(ep, q_rows, 128), held(ep, cap, width),
            pltpu.VMEM((ep, token_count), jnp.float32), pltpu.VMEM((ep, token_count), jnp.float32),
            held(slots, width),
            held(ep, row_count, 128), held(ep, q_rows, 128),
            held(slots + 16, full),
            held(*wg.shape), held(*wu.shape), held(*wd.shape),
            held(tp * channels if wide else channels, full),
            held(slots, full), held(chips, slots, width), held(others, slots, width),
            held(others, slots, width), held(slots, width),
            held(ep, q_rows, 128), held(ep, q_rows, 128), held(row_count, wo.shape[0]),
            held(*((16, 128) if wide else (half, full))),
            held(*((16, 128) if wide else (half, full))),
            held(*((1, 16, 128) if wide else (chips, half, full))),
            held(*((half, tp * channels) if wide else (16, 128))),
            held(ep, token_count, 2 * cap),
        ]
        + both(ep) + [dma((ep,))] + both(ep) + both(ep) + both(ep + 1) + both(chips, ep + 1)
        + both(chips, ep + 1) + both(chips, groups) + both(chips, ep) + both(ep) + both(ep)
        + both(1) + both(chips, pieces) + both(pieces) + both(tp) + both(w_pieces)
        + both(w_pieces) + both(4) + [dma((1 + 3 * heads,)), dma((4,))],
        compiler_params=pltpu.CompilerParams(
            collective_id=0, has_side_effects=True, vmem_limit_bytes=60 * 1024 * 1024
        ),
    )(routes, scale, gains, off, exp_rows, mix, wq, wk, wv, wg, wu, wd, wo)


def on_device(
    mix_rows,
    mix_gain,
    w_query,
    w_key,
    w_value,
    key_offset,
    w_out,
    out_gain,
    exp_rows,
    exp_gain,
    routes,
    route_weight,
    w_gate,
    w_up,
    w_down,
):
    ep = lax.axis_size("ep")
    tp = lax.axis_size("tp")
    row_count = mix_rows.shape[0]
    heads_here = key_offset.shape[0]
    head_size = w_query.shape[0] // heads_here
    share = ep // heads_here
    part = row_count // share
    packed = part % 32 == 0 and heads_here % 2 == 0
    token_count, top_count = routes.shape
    experts = w_gate.shape[0] * ep
    capacity = 4 * token_count * top_count // (3 * experts)
    gains = jnp.concatenate([mix_gain, out_gain, exp_gain]).astype(jnp.float32)
    if not packed:
        w_out = w_out.reshape(heads_here, head_size, -1)
        w_out = jnp.concatenate([jnp.zeros_like(w_out), w_out], axis=1)
        w_out = w_out.reshape(2 * heads_here * head_size, -1)
    mix_out, exp_out = one_call(
        ep, tp, share, part, packed, capacity, routes.T, route_weight.T, gains, key_offset,
        exp_rows, mix_rows, w_query, w_key, w_value, w_gate[0], w_up[0], w_down[0], w_out,
    )
    return (mix_out, exp_out)


def solution(mesh):
    placed = (
        P("ep", None),
        P(),
        P("tp", None),
        P("tp", None),
        P("tp", None),
        P("tp", None),
        P("tp", None),
        P(),
        P("ep", "tp"),
        P("tp"),
        P("ep", None),
        P("ep", None),
        P("ep", None, "tp"),
        P("ep", None, "tp"),
        P("ep", "tp", None),
    )
    return jax.shard_map(
        on_device,
        mesh=mesh,
        in_specs=placed,
        out_specs=(P("ep", None), P("ep", "tp")),
        check_vma=False,
    )
```
